32 devices in a mesh: grp: 2 (over y), sp: 4 (over z), tp: 4 (over x, core).
Axes of the slice: x: 2, y: 2, z: 4, core: 2. Of those that a mesh axis runs over, the one named last changes fastest.
Arguments:
- ssm_input: bfloat16 [1024, 1024], P(('grp', 'sp'), 'tp'), parts along dimension 0, may hold values from -6 to 6
- residual_in: bfloat16 [1024, 2048], P(('grp', 'sp')), parts along dimension 0, may hold values from -4 to 4
- log_step: float32 [64], P('tp'), may hold values from -6.91 to -2.3
- decay_real: float32 [64, 64], P('tp'), may hold values from -34 to 0, as said below
- freq: float32 [64, 64], P('tp'), may hold values from 0.5 to 8
- in_real: float32 [64, 64, 16], P('tp'), may hold values from -1 to 1
- in_imag: float32 [64, 64, 16], P('tp'), may hold values from -1 to 1
- out_real: float32 [64, 16, 64], P('tp'), may hold values from -0.5 to 0.5
- out_imag: float32 [64, 16, 64], P('tp'), may hold values from -0.5 to 0.5
- skip: float32 [1024], P('tp'), may hold values from -3 to 3
- w_glu: bfloat16 [1024, 1024], replicated, may hold values from -0.1875 to 0.1875
- b_glu: float32 [1024], replicated, may hold values from -3 to 3
- w_branch: bfloat16 [1024, 2048], replicated, may hold values from -0.1875 to 0.1875
- norm_gain: float32 [2048], replicated, may hold values from 0.1 to 1.9
- w_gate: bfloat16 [2048, 5632], P('sp', 'tp'), may hold values from -0.125 to 0.125
- w_up: bfloat16 [2048, 5632], P('sp', 'tp'), may hold values from -0.125 to 0.125
- w_down: bfloat16 [5632, 2048], P('tp', 'sp'), may hold values from -0.078125 to 0.078125
Outputs:
- mixed: bfloat16 [1024, 2048], P(('grp', 'sp', 'tp')), parts along dimension 0
The draws below stay inside these ranges and needn't reach their ends.
There are 2 independent parts, one for each index of `grp`. The reference program is written for one: setup_inputs(seed, part) draws one part's arguments, and reference() takes and returns one part's arrays. A program takes and returns all parts, laid end to end along the dimension named above; an argument that names none is the same for every part. Nothing has to cross between parts.
Inputs may be any that keep to these rules, and one draw needn't show every extreme that they name: `decay_real`: negative in every entry.
All inputs are finite; a program needn't handle non-finite values.
Results may differ from the reference program's by a relative error of at most 0.015.
Values may be sent and summed in bfloat16 or wider, within the bound.
No kernel may reach another device: no remote copies, remote signals or barrier semaphores. Data moves between devices by JAX's collectives and lax.ppermute only.
A program may use at most 128 MiB of HBM per device.

```python
import math
import jax
import jax.numpy as jnp
from jax import lax

D = 2048
FF = 5632
SSM_GROUPS = 64
SSM_GROUP = 16
SSM_STATE = 64
TOK_DEV = 128
SSM_WIDTH = 1024
TOKENS = 512
N_SP = 4


def decay_plan(key):
    subkeys = jax.random.split(jax.random.fold_in(key, 11), 5)
    fast_share = 0.5
    fast_group = jax.random.uniform(subkeys[0], (SSM_GROUPS,), jnp.float32) < fast_share
    slow_rate = jax.random.uniform(subkeys[1], (SSM_GROUPS,), jnp.float32, 0.3, 2.0) / TOKENS
    fast_rate = jax.random.uniform(subkeys[2], (SSM_GROUPS,), jnp.float32, 1.0 / 100.0, 1.0 / 30.0)
    decay_rate = jnp.where(fast_group, fast_rate, slow_rate)
    log_steps = jax.random.uniform(subkeys[3], (SSM_GROUPS,), jnp.float32, math.log(0.001), math.log(0.1))
    spread = jax.random.uniform(subkeys[4], (SSM_GROUPS, SSM_STATE), jnp.float32, 0.5, 1.0)
    return (log_steps, decay_rate, spread)


def draw_log_step(key, part):
    return decay_plan(key)[0]


def draw_decay_real(key, part):
    log_steps, decay_rate, spread = decay_plan(key)
    return -decay_rate[:, None] * spread / jnp.exp(log_steps)[:, None]


def shard_levels(rng, shape, pieces, smallest, largest):
    gain = 1.0
    for position, blocks in pieces:
        heights = jax.random.uniform(jax.random.fold_in(jax.random.fold_in(rng, 6), position), (blocks,), jnp.float32, smallest / len(pieces), largest / len(pieces))
        gain = gain * jnp.repeat(jnp.exp(heights), shape[position] // blocks).reshape((-1,) + (1,) * (len(shape) - 1 - position))
    return gain


def centred(own_key, shape, scale, most, cuts=(), kind=jnp.bfloat16):
    result = scale * jax.random.normal(own_key, shape, jnp.float32)
    if cuts:
        result = result * shard_levels(own_key, shape, cuts, -0.22, 0.18)
    return jnp.clip(result, -most, most).astype(kind)


def setup_inputs(seed: int = 0, part: int = 0) -> dict:
    key_of = jax.random.split(jax.random.key(seed), 18)
    own_keys = jax.random.split(jax.random.fold_in(key_of[17], part), 18)
    return {
        "ssm_input": centred(own_keys[0], (TOKENS, SSM_WIDTH), 1.0, 6.0, ((0, 4), (1, 4))),
        "residual_in": centred(own_keys[1], (TOKENS, D), 0.5, 4.0, ((0, 4),)),
        "log_step": draw_log_step(jax.random.fold_in(key_of[17], 71), part),
        "decay_real": draw_decay_real(jax.random.fold_in(key_of[17], 71), part),
        "freq": jnp.clip(0.5 + 7.5 * jax.random.uniform(key_of[4], (SSM_GROUPS, SSM_STATE), jnp.float32) ** shard_levels(key_of[4], (SSM_GROUPS, SSM_STATE), ((0, 4),), -0.2, 0.2), 0.5, 8.0),
        "in_real": centred(key_of[5], (SSM_GROUPS, SSM_STATE, SSM_GROUP), (2 * SSM_GROUP) ** -0.5, 1.0, ((0, 4),), jnp.float32),
        "in_imag": centred(key_of[6], (SSM_GROUPS, SSM_STATE, SSM_GROUP), (2 * SSM_GROUP) ** -0.5, 1.0, ((0, 4),), jnp.float32),
        "out_real": centred(key_of[7], (SSM_GROUPS, SSM_GROUP, SSM_STATE), (2 * SSM_STATE) ** -0.5, 0.5, ((0, 4),), jnp.float32),
        "out_imag": centred(key_of[8], (SSM_GROUPS, SSM_GROUP, SSM_STATE), (2 * SSM_STATE) ** -0.5, 0.5, ((0, 4),), jnp.float32),
        "skip": centred(key_of[9], (SSM_WIDTH,), 0.5, 3.0, ((0, 4),), jnp.float32),
        "w_glu": centred(key_of[10], (SSM_WIDTH, SSM_WIDTH), SSM_WIDTH ** -0.5, 0.1875),
        "b_glu": centred(key_of[11], (SSM_WIDTH,), 0.5, 3.0, (), jnp.float32),
        "w_branch": centred(key_of[12], (SSM_WIDTH, D), SSM_WIDTH ** -0.5, 0.1875),
        "norm_gain": jnp.clip(1.0 + 0.18 * jax.random.normal(key_of[13], (D,), jnp.float32), 0.1, 1.9),
        "w_gate": centred(key_of[14], (D, FF), D ** -0.5, 0.125, ((0, 4), (1, 4))),
        "w_up": centred(key_of[15], (D, FF), D ** -0.5, 0.125, ((0, 4), (1, 4))),
        "w_down": centred(key_of[16], (FF, D), FF ** -0.5, 0.078125, ((0, 4), (1, 4))),
    }


EPS = 1e-06

def discretize(log_step, decay_real, freq, in_real, in_imag):
    step_size = jnp.exp(log_step)[:, None]
    magnitude = jnp.exp(decay_real * step_size)
    abar_re = magnitude * jnp.cos(freq * step_size)
    abar_im = magnitude * jnp.sin(freq * step_size)
    denominator = decay_real * decay_real + freq * freq
    less_re = abar_re - 1.0
    less_im = abar_im
    hold_re = ((less_re * decay_real + less_im * freq) / denominator)[..., None]
    hold_im = ((less_im * decay_real - less_re * freq) / denominator)[..., None]
    bbar_re = hold_re * in_real - hold_im * in_imag
    bbar_im = hold_re * in_imag + hold_im * in_real
    return (step_size, abar_re, abar_im, bbar_re, bbar_im)

def powers(decay_real, freq, step_size, length):
    steps_up = (jnp.arange(length, dtype=jnp.int32) + 1).astype(jnp.float32)[:, None, None]
    magnitude = jnp.exp((decay_real * step_size)[None] * steps_up)
    phase = (freq * step_size)[None] * steps_up
    return (magnitude * jnp.cos(phase), magnitude * jnp.sin(phase))

def compose(earlier, later):
    a1r, a1i, b1r, b1i = earlier
    a2r, a2i, b2r, b2i = later
    return (a2r * a1r - a2i * a1i, a2r * a1i + a2i * a1r, a2r * b1r - a2i * b1i + b2r, a2r * b1i + a2i * b1r + b2i)

def local_states(inputs, abar_re, abar_im, bbar_re, bbar_im):
    hp = lax.Precision.HIGHEST
    drive_re = jnp.einsum('lgm,gpm->lgp', inputs, bbar_re, precision=hp)
    drive_im = jnp.einsum('lgm,gpm->lgp', inputs, bbar_im, precision=hp)
    full_re = jnp.broadcast_to(abar_re[None], drive_re.shape)
    full_im = jnp.broadcast_to(abar_im[None], drive_re.shape)
    scanned = lax.associative_scan(compose, (full_re, full_im, drive_re, drive_im), axis=0)
    return (scanned[2], scanned[3])

def readout(state_re, state_im, out_real, out_imag, skip_mat, inputs):
    hp = lax.Precision.HIGHEST
    values = jnp.einsum('lgp,gmp->lgm', state_re, out_real, precision=hp) - jnp.einsum('lgp,gmp->lgm', state_im, out_imag, precision=hp) + skip_mat[None] * inputs
    values = jax.nn.gelu(values)
    return values.reshape(values.shape[0], -1).astype(jnp.bfloat16)

def reference(ssm_input, residual_in, log_step, decay_real, freq, in_real, in_imag, out_real, out_imag, skip, w_glu, b_glu, w_branch, norm_gain, w_gate, w_up, w_down):
    step_size, abar_re, abar_im, bbar_re, bbar_im = discretize(log_step, decay_real, freq, in_real, in_imag)
    pow_re, pow_im = powers(decay_real, freq, step_size, TOK_DEV)
    skip_mat = skip.reshape(SSM_GROUPS, SSM_GROUP)
    blocks = ssm_input.astype(jnp.float32).reshape(N_SP, TOK_DEV, SSM_GROUPS, SSM_GROUP)

    def one_block(carried, inputs):
        local_re, local_im = local_states(inputs, abar_re, abar_im, bbar_re, bbar_im)
        state_re = local_re + pow_re * carried[0][None] - pow_im * carried[1][None]
        state_im = local_im + pow_re * carried[1][None] + pow_im * carried[0][None]
        mixer_out = readout(state_re, state_im, out_real, out_imag, skip_mat, inputs)
        return ((state_re[-1], state_im[-1]), mixer_out)
    start_state = (jnp.zeros((SSM_GROUPS, SSM_STATE), jnp.float32), jnp.zeros((SSM_GROUPS, SSM_STATE), jnp.float32))
    unused, outputs = lax.scan(one_block, start_state, blocks)
    mixer_out = outputs.reshape(TOKENS, SSM_WIDTH)
    glu_pre = jnp.dot(mixer_out, w_glu, preferred_element_type=jnp.float32) + b_glu
    gated = (mixer_out.astype(jnp.float32) * jax.nn.sigmoid(glu_pre)).astype(jnp.bfloat16)
    stream = residual_in.astype(jnp.float32) + jnp.dot(gated, w_branch, preferred_element_type=jnp.float32)
    scale_rows = lax.rsqrt(lax.optimization_barrier(jnp.mean(stream * stream, axis=-1, keepdims=True)) + EPS)
    normed = (stream * scale_rows * norm_gain).astype(jnp.bfloat16)
    gate_sum = jnp.dot(normed, w_gate, preferred_element_type=jnp.float32)
    up_sum = jnp.dot(normed, w_up, preferred_element_type=jnp.float32)
    hidden = (jax.nn.silu(gate_sum) * up_sum).astype(jnp.bfloat16)
    return (stream + jnp.dot(hidden, w_down, preferred_element_type=jnp.float32)).astype(jnp.bfloat16)
```

```python
import math

import jax
import jax.numpy as jnp
from jax import lax
from jax.sharding import PartitionSpec as P

EPS = 1e-06


def prefix(shard, axis, combine, identity):
    count, place = (lax.axis_size(axis), lax.axis_index(axis))
    everything = tuple(jnp.moveaxis(lax.all_gather(jnp.stack(shard), axis), 1, 0))
    start = jax.tree.map(
        lambda part, zero: jnp.broadcast_to(jnp.asarray(zero, part.dtype), part.shape),
        shard,
        identity,
    )

    def lap(k, before):
        reached = k < place
        new = combine(before, tuple(part[k] for part in everything))
        return jax.tree.map(lambda a, b: jnp.where(reached, a, b), new, before)

    return lax.fori_loop(0, count, lap, start)


def discretize(log_step, decay_real, freq, in_real, in_imag):
    step_size = jnp.exp(log_step)[:, None]
    magnitude = jnp.exp(decay_real * step_size)
    abar_re = magnitude * jnp.cos(freq * step_size)
    abar_im = magnitude * jnp.sin(freq * step_size)
    denominator = decay_real * decay_real + freq * freq
    less_re = abar_re - 1.0
    hold_re = ((less_re * decay_real + abar_im * freq) / denominator)[..., None]
    hold_im = ((abar_im * decay_real - less_re * freq) / denominator)[..., None]
    bbar_re = hold_re * in_real - hold_im * in_imag
    bbar_im = hold_re * in_imag + hold_im * in_real
    return (step_size, abar_re, abar_im, bbar_re, bbar_im)


def powers(decay_real, freq, step_size, length):
    steps_up = (jnp.arange(length, dtype=jnp.int32) + 1).astype(jnp.float32)[:, None, None]
    magnitude = jnp.exp((decay_real * step_size)[None] * steps_up)
    phase = (freq * step_size)[None] * steps_up
    return (magnitude * jnp.cos(phase), magnitude * jnp.sin(phase))


def compose(earlier, later):
    a1r, a1i, b1r, b1i = earlier
    a2r, a2i, b2r, b2i = later
    return (
        a2r * a1r - a2i * a1i,
        a2r * a1i + a2i * a1r,
        a2r * b1r - a2i * b1i + b2r,
        a2r * b1i + a2i * b1r + b2i,
    )


def local_states(inputs, decay_real, freq, step_size, bbar_re, bbar_im):
    highest = lax.Precision.HIGHEST
    tok_rows, group_count, unused = inputs.shape
    lanes = group_count * decay_real.shape[1]
    drive_re = jnp.einsum("lgm,gpm->lgp", inputs, bbar_re, precision=highest).reshape(
        tok_rows, lanes
    )
    drive_im = jnp.einsum("lgm,gpm->lgp", inputs, bbar_im, precision=highest).reshape(
        tok_rows, lanes
    )
    span = math.gcd(tok_rows, 16)
    spans = tok_rows // span
    rate = (decay_real * step_size).reshape(lanes)
    turn = (freq * step_size).reshape(lanes)
    later = jnp.arange(span, dtype=jnp.int32)[:, None]
    earlier = jnp.arange(span, dtype=jnp.int32)[None, :]
    lag = (later - earlier).astype(jnp.float32)
    causal = (later >= earlier)[..., None]
    lag_pos = jnp.maximum(lag, 0.0)[..., None]
    table_mag = jnp.exp(rate[None, None] * lag_pos)
    table_re = jnp.where(causal, table_mag * jnp.cos(turn[None, None] * lag_pos), 0.0)
    table_im = jnp.where(causal, table_mag * jnp.sin(turn[None, None] * lag_pos), 0.0)
    block_re = drive_re.reshape(spans, 1, span, lanes)
    block_im = drive_im.reshape(spans, 1, span, lanes)
    inner_re = jnp.sum(table_re[None] * block_re - table_im[None] * block_im, axis=2)
    inner_im = jnp.sum(table_re[None] * block_im + table_im[None] * block_re, axis=2)
    steps_up = (jnp.arange(span, dtype=jnp.int32) + 1).astype(jnp.float32)[:, None]
    pow_mag = jnp.exp(rate[None] * steps_up)
    pow_re = pow_mag * jnp.cos(turn[None] * steps_up)
    pow_im = pow_mag * jnp.sin(turn[None] * steps_up)
    span_re = pow_re[-1]
    span_im = pow_im[-1]

    def carry_step(entering, ends):
        next_re = span_re * entering[0] - span_im * entering[1] + ends[0]
        next_im = span_re * entering[1] + span_im * entering[0] + ends[1]
        return ((next_re, next_im), entering)

    zeros = jnp.zeros((lanes,), jnp.float32)
    unused_carry, entering = lax.scan(
        carry_step, (zeros, zeros), (inner_re[:, -1], inner_im[:, -1])
    )
    state_re = inner_re + pow_re[None] * entering[0][:, None] - pow_im[None] * entering[1][:, None]
    state_im = inner_im + pow_re[None] * entering[1][:, None] + pow_im[None] * entering[0][:, None]
    shape = (tok_rows, group_count, decay_real.shape[1])
    return (state_re.reshape(shape), state_im.reshape(shape))


def readout(state_re, state_im, out_real, out_imag, skip_mat, inputs):
    highest = lax.Precision.HIGHEST
    values = (
        jnp.einsum("lgp,gmp->lgm", state_re, out_real, precision=highest)
        - jnp.einsum("lgp,gmp->lgm", state_im, out_imag, precision=highest)
        + skip_mat[None] * inputs
    )
    values = jax.nn.gelu(values)
    return values.reshape(values.shape[0], -1).astype(jnp.bfloat16)


def row_norm(stream, norm_gain):
    scale_rows = lax.rsqrt(jnp.mean(stream * stream, axis=-1, keepdims=True) + EPS)
    return (stream * scale_rows * norm_gain).astype(jnp.bfloat16)


LANES = 128


def resharded(tok_rows, w_gate, w_down):
    planes, parts, cores = (lax.axis_size("sp"), lax.axis_size("grp"), lax.axis_size("tp"))
    rows, units = w_gate.shape
    width = tile_width(units, planes)
    return (
        1 < planes <= 8
        and parts == 2
        and cores == 4
        and units >= width
        and rows % 32 == 0
        and tok_rows % (cores * 16) == 0
    )


def tile_width(units, planes):
    return -(-(-(-units // planes)) // LANES) * LANES


def hop(value, axis, distance):
    count = lax.axis_size(axis)
    return lax.ppermute(value, axis, [(i, (i + distance) % count) for i in range(count)])


def swap(value, axis, bit):
    return lax.ppermute(value, axis, [(i, i ^ bit) for i in range(lax.axis_size(axis))])


def reshard(w_gate, w_up, w_down):
    planes, place, part = (lax.axis_size("sp"), lax.axis_index("sp"), lax.axis_index("grp"))
    rows, units = w_gate.shape
    cols = w_down.shape[1]
    width = tile_width(units, planes)
    half_rows, half_width = (rows // 2, width // 2)

    def start(plane):
        return jnp.minimum(plane * width, units - width)

    wide = jnp.zeros((planes * rows, 2 * width), w_gate.dtype)
    tall = jnp.zeros((width, planes * cols), w_down.dtype)
    own = start(place)
    mine = jnp.concatenate(
        [
            lax.dynamic_slice(w_gate, (0, own), (rows, width)),
            lax.dynamic_slice(w_up, (0, own), (rows, width)),
        ],
        axis=1,
    )
    wide = lax.dynamic_update_slice(wide, mine, (place * rows, 0))
    tall = lax.dynamic_update_slice(
        tall, lax.dynamic_slice(w_down, (own, 0), (width, cols)), (0, place * cols)
    )
    for distance in range(1, planes):
        target = start((place + distance) % planes)
        source = (place - distance) % planes
        piece = jnp.concatenate(
            [
                lax.dynamic_slice(w_gate, (part * half_rows, target), (half_rows, width)),
                lax.dynamic_slice(w_up, (part * half_rows, target), (half_rows, width)),
            ],
            axis=1,
        )
        piece = hop(piece, "sp", distance)
        other = swap(piece, "grp", 1)
        wide = lax.dynamic_update_slice(wide, piece, (source * rows + part * half_rows, 0))
        wide = lax.dynamic_update_slice(wide, other, (source * rows + (1 - part) * half_rows, 0))
    for distance in range(1, planes):
        target = start((place + distance) % planes)
        source = (place - distance) % planes
        piece = lax.dynamic_slice(w_down, (target + part * half_width, 0), (half_width, cols))
        piece = hop(piece, "sp", distance)
        other = swap(piece, "grp", 1)
        tall = lax.dynamic_update_slice(tall, piece, (part * half_width, source * cols))
        tall = lax.dynamic_update_slice(tall, other, ((1 - part) * half_width, source * cols))
    unit = own + jnp.arange(width, dtype=jnp.int32)
    live = jnp.logical_and(unit >= place * width, place * width < units)
    tall = jnp.where(live[:, None], tall, jnp.zeros_like(tall))
    return (wide, tall)


def hidden_sums(normed, w_gate, w_up, w_down):
    planes = lax.axis_size("sp")
    own_rows = normed.shape[0]
    wide, tall = reshard(w_gate, w_up, w_down)
    width = tall.shape[0]
    tokens = jnp.concatenate([normed] + [hop(normed, "sp", d) for d in range(1, planes)], axis=0)
    tokens = jnp.concatenate([tokens, swap(tokens, "tp", 2)], axis=0)
    tokens = jnp.concatenate([tokens, swap(tokens, "tp", 1)], axis=0)
    sums = jnp.dot(tokens, wide, preferred_element_type=jnp.float32)
    hidden = (jax.nn.silu(sums[:, :width]) * sums[:, width:]).astype(jnp.bfloat16)
    part = jnp.dot(hidden, tall, preferred_element_type=jnp.float32)
    for bit in (1, 2):
        half = part.shape[0] // 2
        sent = swap(part[half:].astype(jnp.bfloat16), "tp", bit)
        part = part[:half] + sent.astype(jnp.float32)
    blocks = part.astype(jnp.bfloat16).reshape(planes, own_rows, -1)
    total = part[:own_rows]
    for d in range(1, planes):
        total = total + hop(blocks[d], "sp", -d).astype(jnp.float32)
    return total


def per_device(
    ssm_input,
    residual_in,
    log_step,
    decay_real,
    freq,
    in_real,
    in_imag,
    out_real,
    out_imag,
    skip,
    w_glu,
    b_glu,
    w_branch,
    norm_gain,
    w_gate,
    w_up,
    w_down,
):
    tok_rows, width_local = ssm_input.shape
    group_count = log_step.shape[0]
    group_size = in_real.shape[2]
    tp_count = lax.axis_size("tp")
    tp_index = lax.axis_index("tp")
    own_rows = tok_rows // tp_count
    step_size, abar_re, abar_im, bbar_re, bbar_im = discretize(
        log_step, decay_real, freq, in_real, in_imag
    )
    pow_re, pow_im = powers(decay_real, freq, step_size, tok_rows)
    inputs = ssm_input.astype(jnp.float32).reshape(tok_rows, group_count, group_size)
    local_re, local_im = local_states(inputs, decay_real, freq, step_size, bbar_re, bbar_im)
    identity = (
        jnp.ones_like(abar_re),
        jnp.zeros_like(abar_re),
        jnp.zeros_like(abar_re),
        jnp.zeros_like(abar_re),
    )
    carried = prefix((pow_re[-1], pow_im[-1], local_re[-1], local_im[-1]), "sp", compose, identity)
    state_re = local_re + pow_re * carried[2][None] - pow_im * carried[3][None]
    state_im = local_im + pow_re * carried[3][None] + pow_im * carried[2][None]
    mixer_out = readout(
        state_re, state_im, out_real, out_imag, skip.reshape(group_count, group_size), inputs
    )
    mixer_rows = lax.all_to_all(mixer_out, "tp", split_axis=0, concat_axis=1, tiled=True)
    glu_pre = jnp.dot(mixer_rows, w_glu, preferred_element_type=jnp.float32) + b_glu
    gated = (mixer_rows.astype(jnp.float32) * jax.nn.sigmoid(glu_pre)).astype(jnp.bfloat16)
    residual_own = lax.dynamic_slice_in_dim(residual_in, tp_index * own_rows, own_rows, 0)
    stream = residual_own.astype(jnp.float32) + jnp.dot(
        gated, w_branch, preferred_element_type=jnp.float32
    )
    normed = row_norm(stream, norm_gain)
    if resharded(tok_rows, w_gate, w_down):
        summed = hidden_sums(normed, w_gate, w_up, w_down)
        return (stream + summed).astype(jnp.bfloat16)
    normed_all = lax.all_gather(normed, "tp", axis=0, tiled=True)
    gate_sum = jnp.dot(
        normed_all,
        lax.all_gather(w_gate, "sp", axis=0, tiled=True),
        preferred_element_type=jnp.float32,
    )
    up_sum = jnp.dot(
        normed_all,
        lax.all_gather(w_up, "sp", axis=0, tiled=True),
        preferred_element_type=jnp.float32,
    )
    hidden = (jax.nn.silu(gate_sum) * up_sum).astype(jnp.bfloat16)
    down_whole = lax.all_gather(w_down, "sp", axis=1, tiled=True)
    summed = lax.psum_scatter(
        jnp.dot(hidden, down_whole, preferred_element_type=jnp.float32).astype(jnp.bfloat16),
        "tp",
        scatter_dimension=0,
        tiled=True,
    ).astype(jnp.float32)
    return (stream + summed).astype(jnp.bfloat16)


def solution(mesh):
    placed = (
        P(("grp", "sp"), "tp"),
        P(("grp", "sp"), None),
        P("tp"),
        P("tp", None),
        P("tp", None),
        P("tp", None, None),
        P("tp", None, None),
        P("tp", None, None),
        P("tp", None, None),
        P("tp"),
        P(),
        P(),
        P(),
        P(),
        P("sp", "tp"),
        P("sp", "tp"),
        P("tp", "sp"),
    )
    return jax.shard_map(
        per_device,
        mesh=mesh,
        in_specs=placed,
        out_specs=P(("grp", "sp", "tp"), None),
        check_vma=False,
    )
```

```python
import math

import jax
import jax.numpy as jnp
from jax import lax
from jax.experimental import pallas as pl
from jax.experimental.pallas import tpu as pltpu
from jax.sharding import PartitionSpec as P

EPS = 1e-06


def prefix(shard, axis, combine, identity):
    count, place = (lax.axis_size(axis), lax.axis_index(axis))
    everything = tuple(jnp.moveaxis(lax.all_gather(jnp.stack(shard), axis), 1, 0))
    start = jax.tree.map(
        lambda part, zero: jnp.broadcast_to(jnp.asarray(zero, part.dtype), part.shape),
        shard,
        identity,
    )

    def lap(k, before):
        reached = k < place
        new = combine(before, tuple(part[k] for part in everything))
        return jax.tree.map(lambda a, b: jnp.where(reached, a, b), new, before)

    return lax.fori_loop(0, count, lap, start)


def discretize(log_step, decay_real, freq, in_real, in_imag):
    step_size = jnp.exp(log_step)[:, None]
    magnitude = jnp.exp(decay_real * step_size)
    abar_re = magnitude * jnp.cos(freq * step_size)
    abar_im = magnitude * jnp.sin(freq * step_size)
    denominator = decay_real * decay_real + freq * freq
    less_re = abar_re - 1.0
    hold_re = ((less_re * decay_real + abar_im * freq) / denominator)[..., None]
    hold_im = ((abar_im * decay_real - less_re * freq) / denominator)[..., None]
    bbar_re = hold_re * in_real - hold_im * in_imag
    bbar_im = hold_re * in_imag + hold_im * in_real
    return (step_size, abar_re, abar_im, bbar_re, bbar_im)


def powers(decay_real, freq, step_size, length):
    steps_up = (jnp.arange(length, dtype=jnp.int32) + 1).astype(jnp.float32)[:, None, None]
    magnitude = jnp.exp((decay_real * step_size)[None] * steps_up)
    phase = (freq * step_size)[None] * steps_up
    return (magnitude * jnp.cos(phase), magnitude * jnp.sin(phase))


def compose(earlier, later):
    a1r, a1i, b1r, b1i = earlier
    a2r, a2i, b2r, b2i = later
    return (
        a2r * a1r - a2i * a1i,
        a2r * a1i + a2i * a1r,
        a2r * b1r - a2i * b1i + b2r,
        a2r * b1i + a2i * b1r + b2i,
    )


def local_states(inputs, decay_real, freq, step_size, bbar_re, bbar_im):
    highest = lax.Precision.HIGHEST
    tok_rows, group_count, unused = inputs.shape
    lanes = group_count * decay_real.shape[1]
    drive_re = jnp.einsum("lgm,gpm->lgp", inputs, bbar_re, precision=highest).reshape(
        tok_rows, lanes
    )
    drive_im = jnp.einsum("lgm,gpm->lgp", inputs, bbar_im, precision=highest).reshape(
        tok_rows, lanes
    )
    span = math.gcd(tok_rows, 16)
    spans = tok_rows // span
    rate = (decay_real * step_size).reshape(lanes)
    turn = (freq * step_size).reshape(lanes)
    later = jnp.arange(span, dtype=jnp.int32)[:, None]
    earlier = jnp.arange(span, dtype=jnp.int32)[None, :]
    lag = (later - earlier).astype(jnp.float32)
    causal = (later >= earlier)[..., None]
    lag_pos = jnp.maximum(lag, 0.0)[..., None]
    table_mag = jnp.exp(rate[None, None] * lag_pos)
    table_re = jnp.where(causal, table_mag * jnp.cos(turn[None, None] * lag_pos), 0.0)
    table_im = jnp.where(causal, table_mag * jnp.sin(turn[None, None] * lag_pos), 0.0)
    block_re = drive_re.reshape(spans, 1, span, lanes)
    block_im = drive_im.reshape(spans, 1, span, lanes)
    inner_re = jnp.sum(table_re[None] * block_re - table_im[None] * block_im, axis=2)
    inner_im = jnp.sum(table_re[None] * block_im + table_im[None] * block_re, axis=2)
    steps_up = (jnp.arange(span, dtype=jnp.int32) + 1).astype(jnp.float32)[:, None]
    pow_mag = jnp.exp(rate[None] * steps_up)
    pow_re = pow_mag * jnp.cos(turn[None] * steps_up)
    pow_im = pow_mag * jnp.sin(turn[None] * steps_up)
    span_re = pow_re[-1]
    span_im = pow_im[-1]

    def carry_step(entering, ends):
        next_re = span_re * entering[0] - span_im * entering[1] + ends[0]
        next_im = span_re * entering[1] + span_im * entering[0] + ends[1]
        return ((next_re, next_im), entering)

    zeros = jnp.zeros((lanes,), jnp.float32)
    unused_carry, entering = lax.scan(
        carry_step, (zeros, zeros), (inner_re[:, -1], inner_im[:, -1])
    )
    state_re = inner_re + pow_re[None] * entering[0][:, None] - pow_im[None] * entering[1][:, None]
    state_im = inner_im + pow_re[None] * entering[1][:, None] + pow_im[None] * entering[0][:, None]
    shape = (tok_rows, group_count, decay_real.shape[1])
    return (state_re.reshape(shape), state_im.reshape(shape))


def readout(state_re, state_im, out_real, out_imag, skip_mat, inputs):
    highest = lax.Precision.HIGHEST
    values = (
        jnp.einsum("lgp,gmp->lgm", state_re, out_real, precision=highest)
        - jnp.einsum("lgp,gmp->lgm", state_im, out_imag, precision=highest)
        + skip_mat[None] * inputs
    )
    values = jax.nn.gelu(values)
    return values.reshape(values.shape[0], -1).astype(jnp.bfloat16)


def row_norm(stream, norm_gain):
    scale_rows = lax.rsqrt(jnp.mean(stream * stream, axis=-1, keepdims=True) + EPS)
    return (stream * scale_rows * norm_gain).astype(jnp.bfloat16)


LANES = 128


def can_reshard(tok_rows, group_count, in_shape, w_gate, w_down):
    planes, parts, cores = (lax.axis_size("sp"), lax.axis_size("grp"), lax.axis_size("tp"))
    rows, units = w_gate.shape
    width = tile_width(units, planes)
    return (
        1 < planes <= 8
        and parts == 2
        and cores == 4
        and units >= width
        and rows % (2 * LANES) == 0
        and w_down.shape[1] % (2 * LANES) == 0
        and tok_rows % (cores * 16) == 0
        and tok_rows & (tok_rows - 1) == 0
        and group_count * in_shape[1] % LANES == 0
        and group_count * in_shape[2] % LANES == 0
    )


def tile_width(units, planes):
    return -(-(-(-units // planes)) // LANES) * LANES


def hop(value, axis, distance):
    count = lax.axis_size(axis)
    return lax.ppermute(value, axis, [(i, (i + distance) % count) for i in range(count)])


def swap(value, axis, bit):
    return lax.ppermute(value, axis, [(i, i ^ bit) for i in range(lax.axis_size(axis))])


def halves(value):
    high = value.astype(jnp.bfloat16)
    return (high, (value - high.astype(jnp.float32)).astype(jnp.bfloat16))


def across(a, b):
    return lax.dot_general(a, b, (((1,), (1,)), ((), ())), preferred_element_type=jnp.float32)


def times(a, b):
    return (a[0] * b[0] - a[1] * b[1], a[0] * b[1] + a[1] * b[0])


def repeated(value, copies):
    size = value.shape[1]
    shape = (size, copies * size)
    pick = lax.broadcasted_iota(jnp.int32, shape, 0) == lax.broadcasted_iota(jnp.int32, shape, 1) % size
    return jnp.dot(value, pick.astype(jnp.bfloat16), preferred_element_type=jnp.float32)


def block_diagonal(value, groups):
    rows, size = (value.shape[0] // groups, value.shape[1])
    shape = (value.shape[0], groups * size)
    own = lax.broadcasted_iota(jnp.int32, shape, 0) // rows == lax.broadcasted_iota(jnp.int32, shape, 1) // size
    return [jnp.where(own, repeated(part, groups), 0.0).astype(jnp.bfloat16) for part in halves(value)]


def local_scan(ssm_input, log_step, decay_real, freq, in_real, in_imag):
    length = ssm_input.shape[0]
    groups, states, size = in_real.shape
    lanes = groups * states

    def kernel(log_ref, x, decay_ref, freq_ref, in_re, in_im, out_re, out_im, end, abar, hold):
        row = lax.broadcasted_iota(jnp.int32, (groups, states), 0)
        log = jnp.zeros((groups, states), jnp.float32)
        for g in range(groups):
            log = jnp.where(row == g, log_ref[g], log)
        step = jnp.exp(log)
        decay, turn = (decay_ref[...], freq_ref[...])
        magnitude = jnp.exp(decay * step)
        abar_re = magnitude * jnp.cos(turn * step)
        abar_im = magnitude * jnp.sin(turn * step)
        denominator = decay * decay + turn * turn
        less_re = abar_re - 1.0
        hold_re = (less_re * decay + abar_im * turn) / denominator
        hold_im = (abar_im * decay - less_re * turn) / denominator
        shape = (states, lanes)
        pick = lax.broadcasted_iota(jnp.int32, shape, 0) == lax.broadcasted_iota(jnp.int32, shape, 1) % states
        own = lax.broadcasted_iota(jnp.int32, (groups, lanes), 0) == (
            lax.broadcasted_iota(jnp.int32, (groups, lanes), 1) // states
        )
        for target, k, value in ((abar, 0, abar_re), (abar, 1, abar_im), (hold, 0, hold_re), (hold, 1, hold_im)):
            wide = jnp.dot(
                value, pick.astype(jnp.float32), preferred_element_type=jnp.float32, precision=lax.Precision.HIGHEST
            )
            target[k : k + 1, :] = jnp.sum(jnp.where(own, wide, 0.0), axis=0, keepdims=True)
        rows = x[...]
        for target, source in ((out_re, in_re), (out_im, in_im)):
            high, low = block_diagonal(source[...], groups)
            target[...] = across(rows, high) + across(rows, low)
        place = lax.broadcasted_iota(jnp.int32, (length, LANES), 0)
        for first in range(0, lanes, LANES):
            at = slice(first, first + LANES)
            power = (abar[0:1, at], abar[1:2, at])
            state = times((hold[0:1, at], hold[1:2, at]), (out_re[:, at], out_im[:, at]))
            gap = 1
            while gap < length:
                late = place >= gap
                before = tuple(jnp.where(late, pltpu.roll(part, gap, 0), 0.0) for part in state)
                moved = times(power, before)
                state = (state[0] + moved[0], state[1] + moved[1])
                power = times(power, power)
                gap *= 2
            out_re[:, at], out_im[:, at] = state
            end[0:1, at] = state[0][length - 1 :]
            end[1:2, at] = state[1][length - 1 :]

    pair = jax.ShapeDtypeStruct((2, lanes), jnp.float32)
    whole = jax.ShapeDtypeStruct((length, lanes), jnp.float32)
    vmem = pl.BlockSpec(memory_space=pltpu.VMEM)
    return pl.pallas_call(
        kernel,
        in_specs=[pl.BlockSpec(memory_space=pltpu.SMEM)] + [vmem] * 5,
        out_specs=[vmem] * 4,
        out_shape=[whole, whole, pair, pair],
        scratch_shapes=[pltpu.VMEM((2, lanes), jnp.float32)],
        compiler_params=pltpu.CompilerParams(vmem_limit_bytes=48 * 1024 * 1024),
        name="local_scan",
    )(
        log_step,
        ssm_input,
        decay_real,
        freq,
        in_real.reshape(lanes, size),
        in_imag.reshape(lanes, size),
    )


def mixed_out(state_re, state_im, abar, ends, out_real, out_imag, skip, ssm_input):
    length, lanes = state_re.shape
    groups, size, states = out_real.shape
    span = 8

    def kernel(*refs):
        s_re, s_im, abar_ref = refs[:3]
        end_refs = refs[3 : 3 + len(ends)]
        o_re, o_im, skip_ref, x, out = refs[3 + len(ends) : 8 + len(ends)]
        full_re, full_im = refs[8 + len(ends) :]
        for first in range(0, lanes, LANES):
            at = slice(first, first + LANES)
            one = (abar_ref[0:1, at], abar_ref[1:2, at])
            count = lax.broadcasted_iota(jnp.int32, (span, LANES), 0) + 1
            table = (jnp.ones((span, LANES), jnp.float32), jnp.zeros((span, LANES), jnp.float32))
            power, gap = (one, 1)
            while gap < length:
                if gap == span:
                    eight = power
                if gap <= span:
                    more = times(table, power)
                    odd = (count // gap) % 2 == 1
                    table = tuple(jnp.where(odd, a, b) for a, b in zip(more, table))
                power = times(power, power)
                gap *= 2
            carry = None
            for end in reversed(end_refs):
                here = (end[0:1, at], end[1:2, at])
                if carry is None:
                    carry = here
                else:
                    moved = times(power, carry)
                    carry = (here[0] + moved[0], here[1] + moved[1])
            table = times(table, carry)
            for start in range(0, length, span):
                rows = slice(start, start + span)
                full_re[rows, at] = s_re[rows, at] + table[0]
                full_im[rows, at] = s_im[rows, at] + table[1]
                table = times(table, eight)
        re_high, re_low = halves(full_re[...])
        im_high, im_low = halves(full_im[...])
        cre_high, cre_low = block_diagonal(o_re[...], groups)
        cim_high, cim_low = block_diagonal(o_im[...], groups)
        value = across(re_high, cre_high) + across(re_low, cre_high) + across(re_high, cre_low)
        value -= across(im_high, cim_high) + across(im_low, cim_high) + across(im_high, cim_low)
        value += skip_ref[...] * x[...].astype(jnp.float32)
        out[...] = jax.nn.gelu(value).astype(jnp.bfloat16)

    vmem = pl.BlockSpec(memory_space=pltpu.VMEM)
    return pl.pallas_call(
        kernel,
        in_specs=[vmem] * (7 + len(ends)),
        out_specs=vmem,
        out_shape=jax.ShapeDtypeStruct((length, groups * size), jnp.bfloat16),
        scratch_shapes=[pltpu.VMEM((length, lanes), jnp.float32)] * 2,
        compiler_params=pltpu.CompilerParams(vmem_limit_bytes=48 * 1024 * 1024),
        name="mixed_out",
    )(
        state_re,
        state_im,
        abar,
        *ends,
        out_real.reshape(groups * size, states),
        out_imag.reshape(groups * size, states),
        skip.reshape(1, -1),
        ssm_input,
    )


def mixer(ssm_input, log_step, decay_real, freq, in_real, in_imag, out_real, out_imag, skip):
    planes = lax.axis_size("sp")
    state_re, state_im, end, abar = local_scan(ssm_input, log_step, decay_real, freq, in_real, in_imag)
    ends = [lax.ppermute(end, "sp", [(i, i + d) for i in range(planes - d)]) for d in range(1, planes)]
    return mixed_out(state_re, state_im, abar, ends, out_real, out_imag, skip, ssm_input)


def reshard(w_gate, w_up, w_down):
    planes, place, part = (lax.axis_size("sp"), lax.axis_index("sp"), lax.axis_index("grp"))
    rows, units = w_gate.shape
    cols = w_down.shape[1]
    width = tile_width(units, planes)
    half_rows, half_cols = (rows // 2, cols // 2)

    def start(plane):
        return jnp.minimum(plane * width, units - width)

    def both(first, count, unit):
        return jnp.concatenate(
            [lax.dynamic_slice(w, (first, unit), (count, width)) for w in (w_gate, w_up)], axis=1
        )

    own = start(place)
    wide = [(both(0, rows, own), place * rows)]
    tall = [(lax.dynamic_slice(w_down, (own, 0), (width, cols)), place * cols)]
    for distance in range(1, planes):
        target = start((place + distance) % planes)
        source = (place - distance) % planes
        piece = hop(both(part * half_rows, half_rows, target), "sp", distance)
        wide.append((piece, source * rows + part * half_rows))
        wide.append((swap(piece, "grp", 1), source * rows + (1 - part) * half_rows))
    for distance in range(1, planes):
        target = start((place + distance) % planes)
        source = (place - distance) % planes
        piece = lax.dynamic_slice(w_down, (target, part * half_cols), (width, half_cols))
        piece = hop(piece, "sp", distance)
        tall.append((piece, source * cols + part * half_cols))
        tall.append((swap(piece, "grp", 1), source * cols + (1 - part) * half_cols))
    return (wide, tall, jnp.minimum(place * width - own, width))


def feed(tokens, wide, tall, dead, kept):
    count, width = (tokens.shape[0], tall[0][0].shape[0])
    cols = sum(piece.shape[1] for piece, unused in tall)
    n_wide, n_tall = (len(wide), len(tall))
    block = math.gcd(kept, 256)

    def kernel(*refs):
        wide_at, tall_at, dead_at, tok = refs[:4]
        wides = refs[4 : 4 + n_wide]
        talls = refs[4 + n_wide : 4 + n_wide + n_tall]
        out_kept, out_sent = refs[-2:]
        sums = None
        for i in range(n_wide):
            first = pl.multiple_of(wide_at[i], LANES)
            rows = tok[:, pl.ds(first, wides[i].shape[0])]
            term = jnp.dot(rows, wides[i][...], preferred_element_type=jnp.float32)
            sums = term if sums is None else sums + term
        gate, up = (sums[:, :width], sums[:, width:])
        hidden = gate / (1.0 + jnp.exp(-gate)) * up
        unit = lax.broadcasted_iota(jnp.int32, hidden.shape, 1)
        hidden = jnp.where(unit >= dead_at[0], hidden, 0.0).astype(jnp.bfloat16)
        sent = pl.program_id(0) < (count - kept) // block
        for i in range(n_tall):
            first = pl.multiple_of(tall_at[i], LANES)
            at = pl.ds(first, talls[i].shape[1])
            term = jnp.dot(hidden, talls[i][...], preferred_element_type=jnp.float32)

            @pl.when(sent)
            def _():
                out_sent[:, at] = term.astype(jnp.bfloat16)

            @pl.when(jnp.logical_not(sent))
            def _():
                out_kept[:, at] = term

    sends, keeps = ((count - kept) // block, kept // block)
    blocks = sends + keeps
    whole = [pl.BlockSpec(p.shape, lambda i: (0, 0)) for p, unused in wide + tall]
    scalar = pl.BlockSpec(memory_space=pltpu.SMEM)
    return pl.pallas_call(
        kernel,
        grid=(blocks,),
        in_specs=[scalar, scalar, scalar]
        + [pl.BlockSpec((block, tokens.shape[1]), lambda i: ((i + keeps) % blocks, 0))]
        + whole,
        out_specs=[
            pl.BlockSpec((block, cols), lambda i: (jnp.maximum(i - sends, 0), 0)),
            pl.BlockSpec((block, cols), lambda i: (jnp.minimum(i, sends - 1), 0)),
        ],
        out_shape=[
            jax.ShapeDtypeStruct((kept, cols), jnp.float32),
            jax.ShapeDtypeStruct((count - kept, cols), jnp.bfloat16),
        ],
        compiler_params=pltpu.CompilerParams(
            dimension_semantics=("arbitrary",), vmem_limit_bytes=48 * 1024 * 1024
        ),
        name="feed",
    )(
        jnp.stack([at for unused, at in wide]).astype(jnp.int32),
        jnp.stack([at for unused, at in tall]).astype(jnp.int32),
        dead.astype(jnp.int32).reshape(1),
        tokens,
        *[piece for piece, unused in wide + tall],
    )


def hidden_sums(normed, w_gate, w_up, w_down):
    planes = lax.axis_size("sp")
    own_rows = normed.shape[0]
    wide, tall, dead = reshard(w_gate, w_up, w_down)
    tokens = jnp.concatenate([normed] + [hop(normed, "sp", d) for d in range(1, planes)], axis=0)
    tokens = jnp.concatenate([tokens, swap(tokens, "tp", 2)], axis=0)
    tokens = jnp.concatenate([tokens, swap(tokens, "tp", 1)], axis=0)
    part, sent = feed(tokens, wide, tall, dead, tokens.shape[0] // 2)
    part = part + swap(sent, "tp", 1).astype(jnp.float32)
    half = part.shape[0] // 2
    part = part[:half] + swap(part[half:].astype(jnp.bfloat16), "tp", 2).astype(jnp.float32)
    blocks = part.astype(jnp.bfloat16).reshape(planes, own_rows, -1)
    total = part[:own_rows]
    for d in range(1, planes):
        total = total + hop(blocks[d], "sp", -d).astype(jnp.float32)
    return total


def per_device(
    ssm_input,
    residual_in,
    log_step,
    decay_real,
    freq,
    in_real,
    in_imag,
    out_real,
    out_imag,
    skip,
    w_glu,
    b_glu,
    w_branch,
    norm_gain,
    w_gate,
    w_up,
    w_down,
):
    tok_rows, width_local = ssm_input.shape
    group_count = log_step.shape[0]
    group_size = in_real.shape[2]
    tp_count = lax.axis_size("tp")
    tp_index = lax.axis_index("tp")
    own_rows = tok_rows // tp_count
    resharded = can_reshard(tok_rows, group_count, in_real.shape, w_gate, w_down)
    if resharded:
        mixer_out = mixer(
            ssm_input, log_step, decay_real, freq, in_real, in_imag, out_real, out_imag, skip
        )
    else:
        step_size, abar_re, abar_im, bbar_re, bbar_im = discretize(
            log_step, decay_real, freq, in_real, in_imag
        )
        pow_re, pow_im = powers(decay_real, freq, step_size, tok_rows)
        inputs = ssm_input.astype(jnp.float32).reshape(tok_rows, group_count, group_size)
        local_re, local_im = local_states(inputs, decay_real, freq, step_size, bbar_re, bbar_im)
        identity = (
            jnp.ones_like(abar_re),
            jnp.zeros_like(abar_re),
            jnp.zeros_like(abar_re),
            jnp.zeros_like(abar_re),
        )
        carried = prefix((pow_re[-1], pow_im[-1], local_re[-1], local_im[-1]), "sp", compose, identity)
        state_re = local_re + pow_re * carried[2][None] - pow_im * carried[3][None]
        state_im = local_im + pow_re * carried[3][None] + pow_im * carried[2][None]
        mixer_out = readout(
            state_re, state_im, out_real, out_imag, skip.reshape(group_count, group_size), inputs
        )
    mixer_rows = lax.all_to_all(mixer_out, "tp", split_axis=0, concat_axis=1, tiled=True)
    glu_pre = jnp.dot(mixer_rows, w_glu, preferred_element_type=jnp.float32) + b_glu
    gated = (mixer_rows.astype(jnp.float32) * jax.nn.sigmoid(glu_pre)).astype(jnp.bfloat16)
    residual_own = lax.dynamic_slice_in_dim(residual_in, tp_index * own_rows, own_rows, 0)
    stream = residual_own.astype(jnp.float32) + jnp.dot(
        gated, w_branch, preferred_element_type=jnp.float32
    )
    normed = row_norm(stream, norm_gain)
    if resharded:
        summed = hidden_sums(normed, w_gate, w_up, w_down)
        return (stream + summed).astype(jnp.bfloat16)
    normed_all = lax.all_gather(normed, "tp", axis=0, tiled=True)
    gate_sum = jnp.dot(
        normed_all,
        lax.all_gather(w_gate, "sp", axis=0, tiled=True),
        preferred_element_type=jnp.float32,
    )
    up_sum = jnp.dot(
        normed_all,
        lax.all_gather(w_up, "sp", axis=0, tiled=True),
        preferred_element_type=jnp.float32,
    )
    hidden = (jax.nn.silu(gate_sum) * up_sum).astype(jnp.bfloat16)
    down_whole = lax.all_gather(w_down, "sp", axis=1, tiled=True)
    summed = lax.psum_scatter(
        jnp.dot(hidden, down_whole, preferred_element_type=jnp.float32).astype(jnp.bfloat16),
        "tp",
        scatter_dimension=0,
        tiled=True,
    ).astype(jnp.float32)
    return (stream + summed).astype(jnp.bfloat16)


def solution(mesh):
    placed = (
        P(("grp", "sp"), "tp"),
        P(("grp", "sp"), None),
        P("tp"),
        P("tp", None),
        P("tp", None),
        P("tp", None, None),
        P("tp", None, None),
        P("tp", None, None),
        P("tp", None, None),
        P("tp"),
        P(),
        P(),
        P(),
        P(),
        P("sp", "tp"),
        P("sp", "tp"),
        P("tp", "sp"),
    )
    return jax.shard_map(
        per_device,
        mesh=mesh,
        in_specs=placed,
        out_specs=P(("grp", "sp", "tp"), None),
        check_vma=False,
    )
```

```python
import math

import jax
import jax.numpy as jnp
from jax import lax
from jax.experimental import pallas as pl
from jax.experimental.pallas import tpu as pltpu
from jax.sharding import PartitionSpec as P

EPS = 1e-06


def prefix(shard, axis, combine, identity):
    count, place = (lax.axis_size(axis), lax.axis_index(axis))
    everything = tuple(jnp.moveaxis(lax.all_gather(jnp.stack(shard), axis), 1, 0))
    start = jax.tree.map(
        lambda part, zero: jnp.broadcast_to(jnp.asarray(zero, part.dtype), part.shape),
        shard,
        identity,
    )

    def lap(k, before):
        reached = k < place
        new = combine(before, tuple(part[k] for part in everything))
        return jax.tree.map(lambda a, b: jnp.where(reached, a, b), new, before)

    return lax.fori_loop(0, count, lap, start)


def discretize(log_step, decay_real, freq, in_real, in_imag):
    step_size = jnp.exp(log_step)[:, None]
    magnitude = jnp.exp(decay_real * step_size)
    abar_re = magnitude * jnp.cos(freq * step_size)
    abar_im = magnitude * jnp.sin(freq * step_size)
    denominator = decay_real * decay_real + freq * freq
    less_re = abar_re - 1.0
    hold_re = ((less_re * decay_real + abar_im * freq) / denominator)[..., None]
    hold_im = ((abar_im * decay_real - less_re * freq) / denominator)[..., None]
    bbar_re = hold_re * in_real - hold_im * in_imag
    bbar_im = hold_re * in_imag + hold_im * in_real
    return (step_size, abar_re, abar_im, bbar_re, bbar_im)


def powers(decay_real, freq, step_size, length):
    steps_up = (jnp.arange(length, dtype=jnp.int32) + 1).astype(jnp.float32)[:, None, None]
    magnitude = jnp.exp((decay_real * step_size)[None] * steps_up)
    phase = (freq * step_size)[None] * steps_up
    return (magnitude * jnp.cos(phase), magnitude * jnp.sin(phase))


def compose(earlier, later):
    a1r, a1i, b1r, b1i = earlier
    a2r, a2i, b2r, b2i = later
    return (
        a2r * a1r - a2i * a1i,
        a2r * a1i + a2i * a1r,
        a2r * b1r - a2i * b1i + b2r,
        a2r * b1i + a2i * b1r + b2i,
    )


def local_states(inputs, decay_real, freq, step_size, bbar_re, bbar_im):
    highest = lax.Precision.HIGHEST
    tok_rows, group_count, _ = inputs.shape
    lanes = group_count * decay_real.shape[1]
    drive_re = jnp.einsum("lgm,gpm->lgp", inputs, bbar_re, precision=highest).reshape(
        tok_rows, lanes
    )
    drive_im = jnp.einsum("lgm,gpm->lgp", inputs, bbar_im, precision=highest).reshape(
        tok_rows, lanes
    )
    span = math.gcd(tok_rows, 16)
    spans = tok_rows // span
    rate = (decay_real * step_size).reshape(lanes)
    turn = (freq * step_size).reshape(lanes)
    later = jnp.arange(span, dtype=jnp.int32)[:, None]
    earlier = jnp.arange(span, dtype=jnp.int32)[None, :]
    lag = (later - earlier).astype(jnp.float32)
    causal = (later >= earlier)[..., None]
    lag_pos = jnp.maximum(lag, 0.0)[..., None]
    table_mag = jnp.exp(rate[None, None] * lag_pos)
    table_re = jnp.where(causal, table_mag * jnp.cos(turn[None, None] * lag_pos), 0.0)
    table_im = jnp.where(causal, table_mag * jnp.sin(turn[None, None] * lag_pos), 0.0)
    block_re = drive_re.reshape(spans, 1, span, lanes)
    block_im = drive_im.reshape(spans, 1, span, lanes)
    inner_re = jnp.sum(table_re[None] * block_re - table_im[None] * block_im, axis=2)
    inner_im = jnp.sum(table_re[None] * block_im + table_im[None] * block_re, axis=2)
    steps_up = (jnp.arange(span, dtype=jnp.int32) + 1).astype(jnp.float32)[:, None]
    pow_mag = jnp.exp(rate[None] * steps_up)
    pow_re = pow_mag * jnp.cos(turn[None] * steps_up)
    pow_im = pow_mag * jnp.sin(turn[None] * steps_up)
    span_re = pow_re[-1]
    span_im = pow_im[-1]

    def carry_step(entering, ends):
        next_re = span_re * entering[0] - span_im * entering[1] + ends[0]
        next_im = span_re * entering[1] + span_im * entering[0] + ends[1]
        return ((next_re, next_im), entering)

    zeros = jnp.zeros((lanes,), jnp.float32)
    _, entering = lax.scan(
        carry_step, (zeros, zeros), (inner_re[:, -1], inner_im[:, -1])
    )
    state_re = inner_re + pow_re[None] * entering[0][:, None] - pow_im[None] * entering[1][:, None]
    state_im = inner_im + pow_re[None] * entering[1][:, None] + pow_im[None] * entering[0][:, None]
    shape = (tok_rows, group_count, decay_real.shape[1])
    return (state_re.reshape(shape), state_im.reshape(shape))


def readout(state_re, state_im, out_real, out_imag, skip_mat, inputs):
    highest = lax.Precision.HIGHEST
    values = (
        jnp.einsum("lgp,gmp->lgm", state_re, out_real, precision=highest)
        - jnp.einsum("lgp,gmp->lgm", state_im, out_imag, precision=highest)
        + skip_mat[None] * inputs
    )
    values = jax.nn.gelu(values)
    return values.reshape(values.shape[0], -1).astype(jnp.bfloat16)


def row_norm(stream, norm_gain):
    scale_rows = lax.rsqrt(jnp.mean(stream * stream, axis=-1, keepdims=True) + EPS)
    return (stream * scale_rows * norm_gain).astype(jnp.bfloat16)


LANES = 128


def can_reshard(tok_rows, group_count, in_shape, w_gate, w_down):
    planes, parts, cores = (lax.axis_size("sp"), lax.axis_size("grp"), lax.axis_size("tp"))
    rows, units = w_gate.shape
    width = tile_width(units, planes)
    return (
        1 < planes <= 8
        and parts == 2
        and cores == 4
        and units >= width
        and rows % (2 * LANES) == 0
        and w_down.shape[1] % (2 * LANES) == 0
        and tok_rows % (cores * 16) == 0
        and tok_rows & (tok_rows - 1) == 0
        and group_count * in_shape[1] % LANES == 0
        and group_count * in_shape[2] % LANES == 0
    )


def tile_width(units, planes):
    return -(-(-(-units // planes)) // LANES) * LANES


def hop(value, axis, distance):
    count = lax.axis_size(axis)
    return lax.ppermute(value, axis, [(i, (i + distance) % count) for i in range(count)])


def swap(value, axis, bit):
    return lax.ppermute(value, axis, [(i, i ^ bit) for i in range(lax.axis_size(axis))])


def halves(value):
    high = value.astype(jnp.bfloat16)
    return (high, (value - high.astype(jnp.float32)).astype(jnp.bfloat16))


def across(a, b):
    return lax.dot_general(a, b, (((1,), (1,)), ((), ())), preferred_element_type=jnp.float32)


def times(a, b):
    return (a[0] * b[0] - a[1] * b[1], a[0] * b[1] + a[1] * b[0])


def repeated(value, copies):
    size = value.shape[1]
    shape = (size, copies * size)
    pick = lax.broadcasted_iota(jnp.int32, shape, 0) == lax.broadcasted_iota(jnp.int32, shape, 1) % size
    return jnp.dot(value, pick.astype(jnp.bfloat16), preferred_element_type=jnp.float32)


def block_diagonal(value, groups):
    rows, size = (value.shape[0] // groups, value.shape[1])
    shape = (value.shape[0], groups * size)
    own = lax.broadcasted_iota(jnp.int32, shape, 0) // rows == lax.broadcasted_iota(jnp.int32, shape, 1) // size
    return [jnp.where(own, repeated(part, groups), 0.0).astype(jnp.bfloat16) for part in halves(value)]


def local_scan(ssm_input, log_step, decay_real, freq, in_real, in_imag):
    length = ssm_input.shape[0]
    groups, states, size = in_real.shape
    lanes = groups * states

    def kernel(log_ref, x, decay_ref, freq_ref, in_re, in_im, out_re, out_im, end, abar, hold):
        row = lax.broadcasted_iota(jnp.int32, (groups, states), 0)
        log = jnp.zeros((groups, states), jnp.float32)
        for g in range(groups):
            log = jnp.where(row == g, log_ref[g], log)
        step = jnp.exp(log)
        decay, turn = (decay_ref[...], freq_ref[...])
        magnitude = jnp.exp(decay * step)
        abar_re = magnitude * jnp.cos(turn * step)
        abar_im = magnitude * jnp.sin(turn * step)
        denominator = decay * decay + turn * turn
        less_re = abar_re - 1.0
        hold_re = (less_re * decay + abar_im * turn) / denominator
        hold_im = (abar_im * decay - less_re * turn) / denominator
        shape = (states, lanes)
        pick = lax.broadcasted_iota(jnp.int32, shape, 0) == lax.broadcasted_iota(jnp.int32, shape, 1) % states
        own = lax.broadcasted_iota(jnp.int32, (groups, lanes), 0) == (
            lax.broadcasted_iota(jnp.int32, (groups, lanes), 1) // states
        )
        for target, k, value in ((abar, 0, abar_re), (abar, 1, abar_im), (hold, 0, hold_re), (hold, 1, hold_im)):
            wide = jnp.dot(
                value, pick.astype(jnp.float32), preferred_element_type=jnp.float32, precision=lax.Precision.HIGHEST
            )
            target[k : k + 1, :] = jnp.sum(jnp.where(own, wide, 0.0), axis=0, keepdims=True)
        rows = x[...]
        for target, source in ((out_re, in_re), (out_im, in_im)):
            high, low = block_diagonal(source[...], groups)
            target[...] = jnp.dot(rows, high, preferred_element_type=jnp.float32) + jnp.dot(
                rows, low, preferred_element_type=jnp.float32
            )
        place = lax.broadcasted_iota(jnp.int32, (length, LANES), 0)
        for first in range(0, lanes, LANES):
            at = slice(first, first + LANES)
            power = (abar[0:1, at], abar[1:2, at])
            state = times((hold[0:1, at], hold[1:2, at]), (out_re[:, at], out_im[:, at]))
            gap = 1
            while gap < length:
                late = place >= gap
                before = tuple(jnp.where(late, pltpu.roll(part, gap, 0), 0.0) for part in state)
                moved = times(power, before)
                state = (state[0] + moved[0], state[1] + moved[1])
                power = times(power, power)
                gap *= 2
            out_re[:, at], out_im[:, at] = state
            end[0:1, at] = state[0][length - 1 :]
            end[1:2, at] = state[1][length - 1 :]

    pair = jax.ShapeDtypeStruct((2, lanes), jnp.float32)
    whole = jax.ShapeDtypeStruct((length, lanes), jnp.float32)
    vmem = pl.BlockSpec()
    return pl.pallas_call(
        kernel,
        grid=(1,),
        in_specs=[pl.BlockSpec(memory_space=pltpu.SMEM)] + [vmem] * 5,
        out_specs=[vmem] * 4,
        out_shape=[whole, whole, pair, pair],
        scratch_shapes=[pltpu.VMEM((2, lanes), jnp.float32)],
        compiler_params=pltpu.CompilerParams(vmem_limit_bytes=48 * 1024 * 1024),
        name="local_scan",
    )(
        log_step,
        ssm_input,
        decay_real,
        freq,
        jnp.swapaxes(in_real, 1, 2).reshape(groups * size, states),
        jnp.swapaxes(in_imag, 1, 2).reshape(groups * size, states),
    )


def mixed_out(state_re, state_im, abar, ends, out_real, out_imag, skip, ssm_input):
    length, lanes = state_re.shape
    groups, size, states = out_real.shape
    span = 8

    def kernel(*refs):
        s_re, s_im, abar_ref = refs[:3]
        end_refs = refs[3 : 3 + len(ends)]
        o_re, o_im, skip_ref, x, out = refs[3 + len(ends) : 8 + len(ends)]
        full_re, full_im = refs[8 + len(ends) :]
        for first in range(0, lanes, LANES):
            at = slice(first, first + LANES)
            one = (abar_ref[0:1, at], abar_ref[1:2, at])
            count = lax.broadcasted_iota(jnp.int32, (span, LANES), 0) + 1
            table = (jnp.ones((span, LANES), jnp.float32), jnp.zeros((span, LANES), jnp.float32))
            power, gap = (one, 1)
            while gap < length:
                if gap == span:
                    eight = power
                if gap <= span:
                    more = times(table, power)
                    odd = (count // gap) % 2 == 1
                    table = tuple(jnp.where(odd, a, b) for a, b in zip(more, table))
                power = times(power, power)
                gap *= 2
            carry = None
            for end in reversed(end_refs):
                here = (end[0:1, at], end[1:2, at])
                if carry is None:
                    carry = here
                else:
                    moved = times(power, carry)
                    carry = (here[0] + moved[0], here[1] + moved[1])
            table = times(table, carry)
            for start in range(0, length, span):
                rows = slice(start, start + span)
                full_re[rows, at] = s_re[rows, at] + table[0]
                full_im[rows, at] = s_im[rows, at] + table[1]
                table = times(table, eight)
        re_high, re_low = halves(full_re[...])
        im_high, im_low = halves(full_im[...])
        cre_high, cre_low = block_diagonal(o_re[...], groups)
        cim_high, cim_low = block_diagonal(o_im[...], groups)
        value = across(re_high, cre_high) + across(re_low, cre_high) + across(re_high, cre_low)
        value -= across(im_high, cim_high) + across(im_low, cim_high) + across(im_high, cim_low)
        value += skip_ref[...] * x[...].astype(jnp.float32)
        out[...] = jax.nn.gelu(value).astype(jnp.bfloat16)

    vmem = pl.BlockSpec()
    return pl.pallas_call(
        kernel,
        grid=(1,),
        in_specs=[vmem] * (7 + len(ends)),
        out_specs=vmem,
        out_shape=jax.ShapeDtypeStruct((length, groups * size), jnp.bfloat16),
        scratch_shapes=[pltpu.VMEM((length, lanes), jnp.float32)] * 2,
        compiler_params=pltpu.CompilerParams(vmem_limit_bytes=48 * 1024 * 1024),
        name="mixed_out",
    )(
        state_re,
        state_im,
        abar,
        *ends,
        out_real.reshape(groups * size, states),
        out_imag.reshape(groups * size, states),
        skip.reshape(1, -1),
        ssm_input,
    )


def mixer(ssm_input, log_step, decay_real, freq, in_real, in_imag, out_real, out_imag, skip):
    planes = lax.axis_size("sp")
    state_re, state_im, end, abar = local_scan(ssm_input, log_step, decay_real, freq, in_real, in_imag)
    ends = []
    for d in range(1, planes):
        ends.append(lax.ppermute(end, "sp", [(i, i + d) for i in range(planes - d)]))
    return mixed_out(state_re, state_im, abar, ends, out_real, out_imag, skip, ssm_input)


def cut(w_gate, w_up, w_down, firsts, part):
    rows, units = w_gate.shape
    cols = w_down.shape[1]
    count = len(firsts)
    width = tile_width(units, lax.axis_size("sp"))

    def kernel(at, gate, up, down, *refs):
        wides, talls, sems = (refs[:count], refs[count : 2 * count], refs[2 * count])
        row = pl.ds(pl.multiple_of(at[count] * (rows // 2), LANES), rows // 2)
        col = pl.ds(pl.multiple_of(at[count] * (cols // 2), LANES), cols // 2)
        copies = []
        for i in range(count):
            unit = pl.ds(pl.multiple_of(at[i], LANES), width)
            copies += [
                (gate.at[row, unit], wides[i].at[:, pl.ds(0, width)]),
                (up.at[row, unit], wides[i].at[:, pl.ds(width, width)]),
                (down.at[unit, col], talls[i]),
            ]
        copies = [pltpu.make_async_copy(a, b, sems.at[i]) for i, (a, b) in enumerate(copies)]
        for copy in copies:
            copy.start()
        for copy in copies:
            copy.wait()

    anywhere = pl.BlockSpec(memory_space=pltpu.HBM)
    pieces = pl.pallas_call(
        kernel,
        in_specs=[pl.BlockSpec(memory_space=pltpu.SMEM)] + [anywhere] * 3,
        out_specs=[pl.BlockSpec(memory_space=pltpu.VMEM)] * (2 * count),
        out_shape=[jax.ShapeDtypeStruct((rows // 2, 2 * width), w_gate.dtype)] * count
        + [jax.ShapeDtypeStruct((width, cols // 2), w_down.dtype)] * count,
        scratch_shapes=[pltpu.SemaphoreType.DMA((3 * count,))],
        name="cut",
    )(jnp.stack([*firsts, part]).astype(jnp.int32), w_gate, w_up, w_down)
    return (pieces[:count], pieces[count:])


def reshard(w_gate, w_up, w_down):
    planes, place, part = (lax.axis_size("sp"), lax.axis_index("sp"), lax.axis_index("grp"))
    units = w_gate.shape[1]
    width = tile_width(units, planes)
    firsts = [
        jnp.minimum((place + d) % planes * width, units - width) for d in range(1, planes)
    ]
    wides, talls = cut(w_gate, w_up, w_down, firsts, part)
    halves_of = []
    for pieces in (wides, talls):
        both = []
        for i, piece in enumerate(pieces):
            piece = hop(piece, "sp", i + 1)
            both.append((piece, swap(piece, "grp", 1)))
        halves_of.append(both)
    return halves_of


def feed(tokens, w_gate, w_up, w_down, wides, talls, kept):
    planes, place, part = (lax.axis_size("sp"), lax.axis_index("sp"), lax.axis_index("grp"))
    count, features = tokens.shape
    rows, units = w_gate.shape
    down_cols = w_down.shape[1]
    width = tile_width(units, planes)
    cols = planes * down_cols
    half_rows, half_cols = (rows // 2, down_cols // 2)
    block = math.gcd(kept, 256)
    sends, keeps = ((count - kept) // block, kept // block)
    blocks = sends + keeps
    wide_list = [half for pair in wides for half in pair]
    tall_list = [half for pair in talls for half in pair]
    n = len(wide_list)
    own = jnp.minimum(place * width, units - width)
    scalars = [own, jnp.minimum(place * width - own, width), place]
    scalars += [
        (place - d) % planes * 2 + (part if half == 0 else 1 - part)
        for d in range(1, planes)
        for half in range(2)
    ]

    def kernel(at, tok, gate, up, down, *refs):
        wide_refs, tall_refs = (refs[:n], refs[n : 2 * n])
        out_kept, out_sent, wide, tall, sems = refs[2 * n :]
        unit = pl.ds(pl.multiple_of(at[0], LANES), width)
        own_rows = pl.ds(pl.multiple_of(at[2] * rows, LANES), rows)
        own_cols = pl.ds(pl.multiple_of(at[2] * down_cols, LANES), down_cols)
        first_copies = [
            (gate.at[:, unit], wide.at[own_rows, pl.ds(0, width)]),
            (up.at[:, unit], wide.at[own_rows, pl.ds(width, width)]),
        ]
        then_copies = [(down.at[unit, :], tall.at[:, own_cols])]
        for i in range(n):
            row = pl.ds(pl.multiple_of(at[3 + i] * half_rows, LANES), half_rows)
            col = pl.ds(pl.multiple_of(at[3 + i] * half_cols, LANES), half_cols)
            first_copies.append((wide_refs[i], wide.at[row, :]))
            then_copies.append((tall_refs[i], tall.at[:, col]))
        copies = [
            pltpu.make_async_copy(a, b, sems.at[i]) for i, (a, b) in enumerate(first_copies + then_copies)
        ]
        start = pl.program_id(0) == 0

        @pl.when(start)
        def _():
            for copy in copies:
                copy.start()
            for copy in copies[: len(first_copies)]:
                copy.wait()

        sums = jnp.dot(tok[...], wide[...], preferred_element_type=jnp.float32)
        gated, upped = (sums[:, :width], sums[:, width:])
        hidden = gated / (1.0 + jnp.exp(-gated)) * upped
        live = lax.broadcasted_iota(jnp.int32, hidden.shape, 1) >= at[1]
        hidden = jnp.where(live, hidden, 0.0).astype(jnp.bfloat16)

        @pl.when(start)
        def _():
            for copy in copies[len(first_copies) :]:
                copy.wait()

        out = jnp.dot(hidden, tall[...], preferred_element_type=jnp.float32)
        sent = pl.program_id(0) < sends

        @pl.when(sent)
        def _():
            out_sent[...] = out.astype(jnp.bfloat16)

        @pl.when(jnp.logical_not(sent))
        def _():
            out_kept[...] = out

    anywhere = pl.BlockSpec(memory_space=pltpu.HBM)
    return pl.pallas_call(
        kernel,
        grid=(blocks,),
        in_specs=[
            pl.BlockSpec(memory_space=pltpu.SMEM),
            pl.BlockSpec((block, features), lambda i: ((i + keeps) % blocks, 0)),
        ]
        + [anywhere] * (3 + 2 * n),
        out_specs=[
            pl.BlockSpec((block, cols), lambda i: (jnp.maximum(i - sends, 0), 0)),
            pl.BlockSpec((block, cols), lambda i: (jnp.minimum(i, sends - 1), 0)),
        ],
        out_shape=[
            jax.ShapeDtypeStruct((kept, cols), jnp.float32),
            jax.ShapeDtypeStruct((count - kept, cols), jnp.bfloat16),
        ],
        scratch_shapes=[
            pltpu.VMEM((planes * rows, 2 * width), w_gate.dtype),
            pltpu.VMEM((width, cols), w_down.dtype),
            pltpu.SemaphoreType.DMA((3 + 2 * n,)),
        ],
        compiler_params=pltpu.CompilerParams(
            dimension_semantics=("arbitrary",), vmem_limit_bytes=48 * 1024 * 1024
        ),
        name="feed",
    )(
        jnp.stack(scalars).astype(jnp.int32),
        tokens,
        w_gate,
        w_up,
        w_down,
        *wide_list,
        *tall_list,
    )


def hidden_sums(normed, w_gate, w_up, w_down, wides, talls):
    planes = lax.axis_size("sp")
    own_rows = normed.shape[0]
    tokens = [normed]
    for d in range(1, planes):
        tokens.append(hop(normed, "sp", d))
    tokens = jnp.concatenate(tokens, axis=0)
    other = swap(tokens, "tp", 2)
    tokens = jnp.concatenate([tokens, other], axis=0)
    other = swap(tokens, "tp", 1)
    tokens = jnp.concatenate([tokens, other], axis=0)
    part, sent = feed(tokens, w_gate, w_up, w_down, wides, talls, tokens.shape[0] // 2)
    part = part + swap(sent, "tp", 1).astype(jnp.float32)
    half = part.shape[0] // 2
    part = part[:half] + swap(part[half:].astype(jnp.bfloat16), "tp", 2).astype(jnp.float32)
    blocks = part.astype(jnp.bfloat16).reshape(planes, own_rows, -1)
    total = part[:own_rows]
    for d in range(1, planes):
        total = total + hop(blocks[d], "sp", -d).astype(jnp.float32)
    return total


def per_device(
    ssm_input,
    residual_in,
    log_step,
    decay_real,
    freq,
    in_real,
    in_imag,
    out_real,
    out_imag,
    skip,
    w_glu,
    b_glu,
    w_branch,
    norm_gain,
    w_gate,
    w_up,
    w_down,
):
    tok_rows, _ = ssm_input.shape
    group_count = log_step.shape[0]
    group_size = in_real.shape[2]
    tp_count = lax.axis_size("tp")
    tp_index = lax.axis_index("tp")
    own_rows = tok_rows // tp_count
    resharded = can_reshard(tok_rows, group_count, in_real.shape, w_gate, w_down)
    if resharded:
        wides, talls = reshard(w_gate, w_up, w_down)
        mixer_out = mixer(
            ssm_input, log_step, decay_real, freq, in_real, in_imag, out_real, out_imag, skip
        )
    else:
        step_size, abar_re, _, bbar_re, bbar_im = discretize(
            log_step, decay_real, freq, in_real, in_imag
        )
        pow_re, pow_im = powers(decay_real, freq, step_size, tok_rows)
        inputs = ssm_input.astype(jnp.float32).reshape(tok_rows, group_count, group_size)
        local_re, local_im = local_states(inputs, decay_real, freq, step_size, bbar_re, bbar_im)
        identity = (
            jnp.ones_like(abar_re),
            jnp.zeros_like(abar_re),
            jnp.zeros_like(abar_re),
            jnp.zeros_like(abar_re),
        )
        carried = prefix((pow_re[-1], pow_im[-1], local_re[-1], local_im[-1]), "sp", compose, identity)
        state_re = local_re + pow_re * carried[2][None] - pow_im * carried[3][None]
        state_im = local_im + pow_re * carried[3][None] + pow_im * carried[2][None]
        mixer_out = readout(
            state_re, state_im, out_real, out_imag, skip.reshape(group_count, group_size), inputs
        )
    mixer_rows = lax.all_to_all(mixer_out, "tp", split_axis=0, concat_axis=1, tiled=True)
    glu_pre = jnp.dot(mixer_rows, w_glu, preferred_element_type=jnp.float32) + b_glu
    gated = (mixer_rows.astype(jnp.float32) * jax.nn.sigmoid(glu_pre)).astype(jnp.bfloat16)
    residual_own = lax.dynamic_slice_in_dim(residual_in, tp_index * own_rows, own_rows, 0)
    stream = residual_own.astype(jnp.float32) + jnp.dot(
        gated, w_branch, preferred_element_type=jnp.float32
    )
    normed = row_norm(stream, norm_gain)
    if resharded:
        summed = hidden_sums(normed, w_gate, w_up, w_down, wides, talls)
        return (stream + summed).astype(jnp.bfloat16)
    normed_all = lax.all_gather(normed, "tp", axis=0, tiled=True)
    gate_sum = jnp.dot(
        normed_all,
        lax.all_gather(w_gate, "sp", axis=0, tiled=True),
        preferred_element_type=jnp.float32,
    )
    up_sum = jnp.dot(
        normed_all,
        lax.all_gather(w_up, "sp", axis=0, tiled=True),
        preferred_element_type=jnp.float32,
    )
    hidden = (jax.nn.silu(gate_sum) * up_sum).astype(jnp.bfloat16)
    down_whole = lax.all_gather(w_down, "sp", axis=1, tiled=True)
    summed = lax.psum_scatter(
        jnp.dot(hidden, down_whole, preferred_element_type=jnp.float32).astype(jnp.bfloat16),
        "tp",
        scatter_dimension=0,
        tiled=True,
    ).astype(jnp.float32)
    return (stream + summed).astype(jnp.bfloat16)


def solution(mesh):
    placed = (
        P(("grp", "sp"), "tp"),
        P(("grp", "sp"), None),
        P("tp"),
        P("tp", None),
        P("tp", None),
        P("tp", None, None),
        P("tp", None, None),
        P("tp", None, None),
        P("tp", None, None),
        P("tp"),
        P(),
        P(),
        P(),
        P(),
        P("sp", "tp"),
        P("sp", "tp"),
        P("tp", "sp"),
    )

    return jax.shard_map(
        per_device,
        mesh=mesh,
        in_specs=placed,
        out_specs=P(("grp", "sp", "tp"), None),
        check_vma=False,
    )
```

```python
import math

import jax
import jax.numpy as jnp
from jax import lax
from jax.experimental import pallas as pl
from jax.experimental.pallas import tpu as pltpu
from jax.sharding import PartitionSpec as P

EPS = 1e-06


def prefix(shard, axis, combine, identity):
    count, place = (lax.axis_size(axis), lax.axis_index(axis))
    everything = tuple(jnp.moveaxis(lax.all_gather(jnp.stack(shard), axis), 1, 0))
    start = jax.tree.map(
        lambda part, zero: jnp.broadcast_to(jnp.asarray(zero, part.dtype), part.shape),
        shard,
        identity,
    )

    def lap(k, before):
        reached = k < place
        new = combine(before, tuple(part[k] for part in everything))
        return jax.tree.map(lambda a, b: jnp.where(reached, a, b), new, before)

    return lax.fori_loop(0, count, lap, start)


def discretize(log_step, decay_real, freq, in_real, in_imag):
    step_size = jnp.exp(log_step)[:, None]
    magnitude = jnp.exp(decay_real * step_size)
    abar_re = magnitude * jnp.cos(freq * step_size)
    abar_im = magnitude * jnp.sin(freq * step_size)
    denominator = decay_real * decay_real + freq * freq
    less_re = abar_re - 1.0
    hold_re = ((less_re * decay_real + abar_im * freq) / denominator)[..., None]
    hold_im = ((abar_im * decay_real - less_re * freq) / denominator)[..., None]
    bbar_re = hold_re * in_real - hold_im * in_imag
    bbar_im = hold_re * in_imag + hold_im * in_real
    return (step_size, abar_re, abar_im, bbar_re, bbar_im)


def powers(decay_real, freq, step_size, length):
    steps_up = (jnp.arange(length, dtype=jnp.int32) + 1).astype(jnp.float32)[:, None, None]
    magnitude = jnp.exp((decay_real * step_size)[None] * steps_up)
    phase = (freq * step_size)[None] * steps_up
    return (magnitude * jnp.cos(phase), magnitude * jnp.sin(phase))


def compose(earlier, later):
    a1r, a1i, b1r, b1i = earlier
    a2r, a2i, b2r, b2i = later
    return (
        a2r * a1r - a2i * a1i,
        a2r * a1i + a2i * a1r,
        a2r * b1r - a2i * b1i + b2r,
        a2r * b1i + a2i * b1r + b2i,
    )


def local_states(inputs, decay_real, freq, step_size, bbar_re, bbar_im):
    highest = lax.Precision.HIGHEST
    tok_rows, group_count, _ = inputs.shape
    lanes = group_count * decay_real.shape[1]
    drive_re = jnp.einsum("lgm,gpm->lgp", inputs, bbar_re, precision=highest).reshape(
        tok_rows, lanes
    )
    drive_im = jnp.einsum("lgm,gpm->lgp", inputs, bbar_im, precision=highest).reshape(
        tok_rows, lanes
    )
    span = math.gcd(tok_rows, 16)
    spans = tok_rows // span
    rate = (decay_real * step_size).reshape(lanes)
    turn = (freq * step_size).reshape(lanes)
    later = jnp.arange(span, dtype=jnp.int32)[:, None]
    earlier = jnp.arange(span, dtype=jnp.int32)[None, :]
    lag = (later - earlier).astype(jnp.float32)
    causal = (later >= earlier)[..., None]
    lag_pos = jnp.maximum(lag, 0.0)[..., None]
    table_mag = jnp.exp(rate[None, None] * lag_pos)
    table_re = jnp.where(causal, table_mag * jnp.cos(turn[None, None] * lag_pos), 0.0)
    table_im = jnp.where(causal, table_mag * jnp.sin(turn[None, None] * lag_pos), 0.0)
    block_re = drive_re.reshape(spans, 1, span, lanes)
    block_im = drive_im.reshape(spans, 1, span, lanes)
    inner_re = jnp.sum(table_re[None] * block_re - table_im[None] * block_im, axis=2)
    inner_im = jnp.sum(table_re[None] * block_im + table_im[None] * block_re, axis=2)
    steps_up = (jnp.arange(span, dtype=jnp.int32) + 1).astype(jnp.float32)[:, None]
    pow_mag = jnp.exp(rate[None] * steps_up)
    pow_re = pow_mag * jnp.cos(turn[None] * steps_up)
    pow_im = pow_mag * jnp.sin(turn[None] * steps_up)
    span_re = pow_re[-1]
    span_im = pow_im[-1]

    def carry_step(entering, ends):
        next_re = span_re * entering[0] - span_im * entering[1] + ends[0]
        next_im = span_re * entering[1] + span_im * entering[0] + ends[1]
        return ((next_re, next_im), entering)

    zeros = jnp.zeros((lanes,), jnp.float32)
    _, entering = lax.scan(
        carry_step, (zeros, zeros), (inner_re[:, -1], inner_im[:, -1])
    )
    state_re = inner_re + pow_re[None] * entering[0][:, None] - pow_im[None] * entering[1][:, None]
    state_im = inner_im + pow_re[None] * entering[1][:, None] + pow_im[None] * entering[0][:, None]
    shape = (tok_rows, group_count, decay_real.shape[1])
    return (state_re.reshape(shape), state_im.reshape(shape))


def readout(state_re, state_im, out_real, out_imag, skip_mat, inputs):
    highest = lax.Precision.HIGHEST
    values = (
        jnp.einsum("lgp,gmp->lgm", state_re, out_real, precision=highest)
        - jnp.einsum("lgp,gmp->lgm", state_im, out_imag, precision=highest)
        + skip_mat[None] * inputs
    )
    values = jax.nn.gelu(values)
    return values.reshape(values.shape[0], -1).astype(jnp.bfloat16)


def row_norm(stream, norm_gain):
    scale_rows = lax.rsqrt(jnp.mean(stream * stream, axis=-1, keepdims=True) + EPS)
    return (stream * scale_rows * norm_gain).astype(jnp.bfloat16)


LANES = 128


def can_reshard(tok_rows, group_count, in_shape, w_gate, w_down):
    planes, parts, cores = (lax.axis_size("sp"), lax.axis_size("grp"), lax.axis_size("tp"))
    rows, units = w_gate.shape
    width = tile_width(units, planes)
    return (
        2 < planes <= 8
        and parts == 2
        and cores == 4
        and units >= width
        and rows % (2 * LANES) == 0
        and w_down.shape[1] % (2 * LANES) == 0
        and tok_rows % (cores * 16) == 0
        and tok_rows & (tok_rows - 1) == 0
        and group_count * in_shape[1] % LANES == 0
        and group_count * in_shape[2] % LANES == 0
    )


def tile_width(units, planes):
    return -(-(-(-units // planes)) // LANES) * LANES


def hop(value, axis, distance):
    count = lax.axis_size(axis)
    return lax.ppermute(value, axis, [(i, (i + distance) % count) for i in range(count)])


def swap(value, axis, bit):
    return lax.ppermute(value, axis, [(i, i ^ bit) for i in range(lax.axis_size(axis))])


def halves(value):
    high = value.astype(jnp.bfloat16)
    return (high, (value - high.astype(jnp.float32)).astype(jnp.bfloat16))


def across(a, b):
    return lax.dot_general(a, b, (((1,), (1,)), ((), ())), preferred_element_type=jnp.float32)


def times(a, b):
    return (a[0] * b[0] - a[1] * b[1], a[0] * b[1] + a[1] * b[0])


def repeated(value, copies):
    size = value.shape[1]
    shape = (size, copies * size)
    pick = lax.broadcasted_iota(jnp.int32, shape, 0) == lax.broadcasted_iota(jnp.int32, shape, 1) % size
    return jnp.dot(value, pick.astype(jnp.bfloat16), preferred_element_type=jnp.float32)


def block_diagonal(value, groups):
    rows, size = (value.shape[0] // groups, value.shape[1])
    shape = (value.shape[0], groups * size)
    own = lax.broadcasted_iota(jnp.int32, shape, 0) // rows == lax.broadcasted_iota(jnp.int32, shape, 1) // size
    return [jnp.where(own, repeated(part, groups), 0.0).astype(jnp.bfloat16) for part in halves(value)]


def local_scan(ssm_input, log_step, decay_real, freq, in_real, in_imag):
    length = ssm_input.shape[0]
    groups, states, size = in_real.shape
    lanes = groups * states

    def kernel(log_ref, x, decay_ref, freq_ref, in_re, in_im, out_re, out_im, end, abar, hold):
        row = lax.broadcasted_iota(jnp.int32, (groups, states), 0)
        log = jnp.zeros((groups, states), jnp.float32)
        for g in range(groups):
            log = jnp.where(row == g, log_ref[g], log)
        step = jnp.exp(log)
        decay, turn = (decay_ref[...], freq_ref[...])
        magnitude = jnp.exp(decay * step)
        abar_re = magnitude * jnp.cos(turn * step)
        abar_im = magnitude * jnp.sin(turn * step)
        denominator = decay * decay + turn * turn
        less_re = abar_re - 1.0
        hold_re = (less_re * decay + abar_im * turn) / denominator
        hold_im = (abar_im * decay - less_re * turn) / denominator
        shape = (states, lanes)
        pick = lax.broadcasted_iota(jnp.int32, shape, 0) == lax.broadcasted_iota(jnp.int32, shape, 1) % states
        own = lax.broadcasted_iota(jnp.int32, (groups, lanes), 0) == (
            lax.broadcasted_iota(jnp.int32, (groups, lanes), 1) // states
        )
        for target, k, value in ((abar, 0, abar_re), (abar, 1, abar_im), (hold, 0, hold_re), (hold, 1, hold_im)):
            wide = jnp.dot(
                value, pick.astype(jnp.float32), preferred_element_type=jnp.float32, precision=lax.Precision.HIGHEST
            )
            target[k : k + 1, :] = jnp.sum(jnp.where(own, wide, 0.0), axis=0, keepdims=True)
        rows = x[...]
        for target, source in ((out_re, in_re), (out_im, in_im)):
            high, low = block_diagonal(source[...], groups)
            target[...] = jnp.dot(rows, high, preferred_element_type=jnp.float32) + jnp.dot(
                rows, low, preferred_element_type=jnp.float32
            )
        place = lax.broadcasted_iota(jnp.int32, (length, LANES), 0)
        for first in range(0, lanes, LANES):
            at = slice(first, first + LANES)
            power = (abar[0:1, at], abar[1:2, at])
            state = times((hold[0:1, at], hold[1:2, at]), (out_re[:, at], out_im[:, at]))
            gap = 1
            while gap < length:
                late = place >= gap
                before = tuple(jnp.where(late, pltpu.roll(part, gap, 0), 0.0) for part in state)
                moved = times(power, before)
                state = (state[0] + moved[0], state[1] + moved[1])
                power = times(power, power)
                gap *= 2
            out_re[:, at], out_im[:, at] = state
            end[0:1, at] = state[0][length - 1 :]
            end[1:2, at] = state[1][length - 1 :]

    pair = jax.ShapeDtypeStruct((2, lanes), jnp.float32)
    whole = jax.ShapeDtypeStruct((length, lanes), jnp.float32)
    vmem = pl.BlockSpec()
    return pl.pallas_call(
        kernel,
        grid=(1,),
        in_specs=[pl.BlockSpec(memory_space=pltpu.SMEM)] + [vmem] * 5,
        out_specs=[vmem] * 4,
        out_shape=[whole, whole, pair, pair],
        scratch_shapes=[pltpu.VMEM((2, lanes), jnp.float32)],
        compiler_params=pltpu.CompilerParams(vmem_limit_bytes=20 * 1024 * 1024),
        name="local_scan",
    )(
        log_step,
        ssm_input,
        decay_real,
        freq,
        jnp.swapaxes(in_real, 1, 2).reshape(groups * size, states),
        jnp.swapaxes(in_imag, 1, 2).reshape(groups * size, states),
    )


def mixed_out(state_re, state_im, abar, ends, out_real, out_imag, skip, ssm_input):
    length, lanes = state_re.shape
    groups, size, states = out_real.shape
    span = 8

    def kernel(*refs):
        s_re, s_im, abar_ref = refs[:3]
        end_refs = refs[3 : 3 + len(ends)]
        o_re, o_im, skip_ref, x, out = refs[3 + len(ends) : 8 + len(ends)]
        full_re, full_im = refs[8 + len(ends) :]
        for first in range(0, lanes, LANES):
            at = slice(first, first + LANES)
            one = (abar_ref[0:1, at], abar_ref[1:2, at])
            count = lax.broadcasted_iota(jnp.int32, (span, LANES), 0) + 1
            table = (jnp.ones((span, LANES), jnp.float32), jnp.zeros((span, LANES), jnp.float32))
            power, gap = (one, 1)
            while gap < length:
                if gap == span:
                    eight = power
                if gap <= span:
                    more = times(table, power)
                    odd = (count // gap) % 2 == 1
                    table = tuple(jnp.where(odd, a, b) for a, b in zip(more, table))
                power = times(power, power)
                gap *= 2
            carry = None
            for end in reversed(end_refs):
                here = (end[0:1, at], end[1:2, at])
                if carry is None:
                    carry = here
                else:
                    moved = times(power, carry)
                    carry = (here[0] + moved[0], here[1] + moved[1])
            table = times(table, carry)
            for start in range(0, length, span):
                rows = slice(start, start + span)
                full_re[rows, at] = s_re[rows, at] + table[0]
                full_im[rows, at] = s_im[rows, at] + table[1]
                table = times(table, eight)
        re_high, re_low = halves(full_re[...])
        im_high, im_low = halves(full_im[...])
        cre_high, cre_low = block_diagonal(o_re[...], groups)
        cim_high, cim_low = block_diagonal(o_im[...], groups)
        value = across(re_high, cre_high) + across(re_low, cre_high) + across(re_high, cre_low)
        value -= across(im_high, cim_high) + across(im_low, cim_high) + across(im_high, cim_low)
        value += skip_ref[...] * x[...].astype(jnp.float32)
        out[...] = jax.nn.gelu(value).astype(jnp.bfloat16)

    vmem = pl.BlockSpec()
    return pl.pallas_call(
        kernel,
        grid=(1,),
        in_specs=[vmem] * (7 + len(ends)),
        out_specs=vmem,
        out_shape=jax.ShapeDtypeStruct((length, groups * size), jnp.bfloat16),
        scratch_shapes=[pltpu.VMEM((length, lanes), jnp.float32)] * 2,
        compiler_params=pltpu.CompilerParams(vmem_limit_bytes=20 * 1024 * 1024),
        name="mixed_out",
    )(
        state_re,
        state_im,
        abar,
        *ends,
        out_real.reshape(groups * size, states),
        out_imag.reshape(groups * size, states),
        skip.reshape(1, -1),
        ssm_input,
    )


def mixer(ssm_input, log_step, decay_real, freq, in_real, in_imag, out_real, out_imag, skip):
    planes = lax.axis_size("sp")
    state_re, state_im, end, abar = local_scan(ssm_input, log_step, decay_real, freq, in_real, in_imag)
    ends = []
    for d in range(1, planes):
        ends.append(lax.ppermute(end, "sp", [(i, i + d) for i in range(planes - d)]))
    return mixed_out(state_re, state_im, abar, ends, out_real, out_imag, skip, ssm_input)


def first_unit(plane, planes, units):
    width = tile_width(units, planes)
    return jnp.minimum(plane * width, units - width)


def run_copies(copies, sems):
    copies = [pltpu.make_async_copy(a, b, sems.at[i]) for i, (a, b) in enumerate(copies)]
    for copy in copies:
        copy.start()
    for copy in copies:
        copy.wait()


def cut(w_gate, w_up, w_down, wide_at, tall_at, grant):
    planes = lax.axis_size("sp")
    rows, units = w_gate.shape
    cols = w_down.shape[1]
    width = tile_width(units, planes)
    count = len(wide_at)

    def kernel(gate, up, down, *refs):
        wides, talls = (refs[:count], refs[count:-1])
        place, part = (lax.axis_index("sp"), lax.axis_index("grp"))
        row = pl.ds(pl.multiple_of(part * (rows // 2), LANES), rows // 2)
        col = pl.ds(pl.multiple_of(part * (cols // 2), LANES), cols // 2)

        def units_of(d):
            first = first_unit((place + d) % planes, planes, units)
            return pl.ds(pl.multiple_of(first, LANES), width)

        copies = []
        for (d, what), wide in zip(wide_at, wides):
            r = row if d else slice(None)
            sources = [w for w, name in ((gate, "gate"), (up, "up")) if what in (name, "both")]
            for i, source in enumerate(sources):
                copies.append((source.at[r, units_of(d)], wide.at[:, pl.ds(i * width, width)]))
        for d, tall in zip(tall_at, talls):
            copies.append((down.at[units_of(d), col if d else slice(None)], tall))
        run_copies(copies, refs[-1])

    anywhere = pl.BlockSpec(memory_space=pltpu.HBM)
    shapes = [
        (rows // 2 if d else rows, 2 * width if what == "both" else width) for d, what in wide_at
    ]
    shapes += [(width, cols // 2 if d else cols) for d in tall_at]
    pieces = pl.pallas_call(
        kernel,
        in_specs=[anywhere] * 3,
        out_specs=[pl.BlockSpec(memory_space=pltpu.VMEM)] * len(shapes),
        out_shape=[jax.ShapeDtypeStruct(shape, w_gate.dtype) for shape in shapes],
        scratch_shapes=[pltpu.SemaphoreType.DMA((2 * count + len(tall_at),))],
        compiler_params=pltpu.CompilerParams(vmem_limit_bytes=grant * 1024 * 1024),
    )(w_gate, w_up, w_down)
    return (dict(zip(wide_at, pieces[:count])), dict(zip(tall_at, pieces[count:])))


def reshard(w_gate, w_up, w_down):
    planes = lax.axis_size("sp")
    order = list(range(1, planes))
    last = order[-1]
    first, unused = cut(w_gate, w_up, w_down, [(1, "both"), (last, "gate")], [], 60)
    middle = [(d, "both") for d in order[1:-1]] + [(last, "up")]
    second, unused = cut(w_gate, w_up, w_down, middle, [], 60)
    third, talls = cut(w_gate, w_up, w_down, [(0, "both")], order + [0], 60)

    def spread(piece, d):
        if d == 0:
            return [(piece, swap(piece, "tp", 1))]
        mine = hop(piece, "sp", d)
        other = swap(mine, "grp", 1)
        return [(half, swap(half, "tp", 1)) for half in (mine, other)]

    wides = []
    for (d, what), piece in {**first, **second, **third}.items():
        wides += [(d, what, half, pair) for half, pair in enumerate(spread(piece, d))]
    return (wides, {d: spread(piece, d) for d, piece in talls.items()})


def gate_up(tokens, wides, core, units):
    planes = lax.axis_size("sp")
    whole = not isinstance(tokens, list)
    toks = [tokens] if whole else tokens
    rows, features = toks[0].shape
    count = rows * len(toks)
    block = features // planes
    width = tile_width(units, planes)
    pieces = [pair[core] for unused_d, unused_what, unused_half, pair in wides]

    def kernel(*refs):
        place, part = (lax.axis_index("sp"), lax.axis_index("grp"))
        spots = []
        for d, what, half, unused in wides:
            start = (place - d + planes) % planes * block
            if d:
                start += (1 - part if half else part) * (block // 2)
            spots.append((start, width if what == "up" else 0))
        tok_refs, weights = (refs[: len(toks)], refs[len(toks) : len(toks) + len(pieces)])
        out, *outs, wide, sems = refs[len(toks) + len(pieces) :]
        tok = tok_refs[0] if whole else outs[0]
        copies = [] if whole else [(ref, tok.at[pl.ds(i * rows, rows), :]) for i, ref in enumerate(tok_refs)]
        for (start, col), weight in zip(spots, weights):
            row = pl.ds(pl.multiple_of(start, 16), weight.shape[0])
            copies.append((weight, wide.at[row, pl.ds(col, weight.shape[1])]))
        run_copies(copies, sems)
        sums = jnp.dot(tok[...], wide[...], preferred_element_type=jnp.float32)
        gate, up = (sums[:, :width], sums[:, width:])
        hidden = gate / (1.0 + jnp.exp(-gate)) * up
        live = lax.broadcasted_iota(jnp.int32, hidden.shape, 1) >= place * width - first_unit(
            place, planes, units
        )
        out[...] = jnp.where(live, hidden, 0.0).astype(jnp.bfloat16)

    anywhere = pl.BlockSpec(memory_space=pl.ANY)
    vmem = pl.BlockSpec(memory_space=pltpu.VMEM)
    shapes = [jax.ShapeDtypeStruct((count, width), jnp.bfloat16)]
    if not whole:
        shapes.append(jax.ShapeDtypeStruct((count, features), jnp.bfloat16))
    return pl.pallas_call(
        kernel,
        in_specs=[vmem if whole else anywhere] * len(toks) + [anywhere] * len(pieces),
        out_specs=[vmem] * len(shapes),
        out_shape=shapes,
        scratch_shapes=[
            pltpu.VMEM((features, 2 * width), jnp.bfloat16),
            pltpu.SemaphoreType.DMA((len(toks) + len(pieces),)),
        ],
        compiler_params=pltpu.CompilerParams(vmem_limit_bytes=16 * 1024 * 1024),
    )(*toks, *pieces)


def down(hiddens, talls, distances):
    count, width = hiddens[0].shape
    pairs = [pair for d in distances for pair in talls[d]]
    flat = [piece for pair in pairs for piece in pair]
    cols = sum(own.shape[1] for own, unused in pairs)
    kept = count // 2

    def kernel(own_hidden, other_hidden, *refs):
        weights = refs[: len(flat)]
        out_kept, out_sent, tall, sems = refs[len(flat) :]
        copies, at = ([], 0)
        for i, (own, unused) in enumerate(pairs):
            col = pl.ds(at, own.shape[1])
            copies += [(weights[2 * i + core], tall.at[core, :, col]) for core in range(2)]
            at += own.shape[1]
        run_copies(copies, sems)

        def product(rows):
            return jnp.dot(
                own_hidden[rows, :], tall[0], preferred_element_type=jnp.float32
            ) + jnp.dot(other_hidden[rows, :], tall[1], preferred_element_type=jnp.float32)

        out_sent[...] = product(slice(kept, count)).astype(jnp.bfloat16)
        out_kept[...] = product(slice(0, kept))

    anywhere = pl.BlockSpec(memory_space=pl.ANY)
    vmem = pl.BlockSpec(memory_space=pltpu.VMEM)
    return pl.pallas_call(
        kernel,
        in_specs=[vmem] * 2 + [anywhere] * len(flat),
        out_specs=[vmem, vmem],
        out_shape=[
            jax.ShapeDtypeStruct((kept, cols), jnp.float32),
            jax.ShapeDtypeStruct((count - kept, cols), jnp.bfloat16),
        ],
        scratch_shapes=[
            pltpu.VMEM((2, width, cols), jnp.bfloat16),
            pltpu.SemaphoreType.DMA((len(flat),)),
        ],
        compiler_params=pltpu.CompilerParams(vmem_limit_bytes=16 * 1024 * 1024),
    )(*hiddens, *flat)


def add_sums(kept, sent, count):
    rows, cols = (kept.shape[0] // count, kept.shape[1])

    def kernel(a, b, *outs):
        for i, out in enumerate(outs):
            at = slice(i * rows, (i + 1) * rows)
            out[...] = (a[at, :] + b[at, :].astype(jnp.float32)).astype(out.dtype)

    vmem = pl.BlockSpec(memory_space=pltpu.VMEM)
    return pl.pallas_call(
        kernel,
        in_specs=[vmem, vmem],
        out_specs=[vmem] * count,
        out_shape=[jax.ShapeDtypeStruct((rows, cols), jnp.float32)]
        + [jax.ShapeDtypeStruct((rows, cols), jnp.bfloat16)] * (count - 1),
        compiler_params=pltpu.CompilerParams(vmem_limit_bytes=8 * 1024 * 1024),
    )(kept, sent)


def gated_branch(blocks, w_glu, b_glu, w_branch, residual_in, norm_gain):
    senders, rows, channels = blocks.shape
    width, features = w_branch.shape

    def kernel(block, bias, gain, glu_hbm, branch_hbm, residual, out_stream, out_normed, mixed, own, glu, branch, sems):
        at = pl.ds(pl.multiple_of(lax.axis_index("tp") * rows, 16), rows)
        copies = [(glu_hbm, glu), (branch_hbm, branch), (residual.at[at, :], own)]
        copies = [pltpu.make_async_copy(a, b, sems.at[i]) for i, (a, b) in enumerate(copies)]
        for copy in copies:
            copy.start()
        for i in range(senders):
            mixed[:, i * channels : (i + 1) * channels] = block[i]
        copies[0].wait()
        pre = jnp.dot(mixed[...], glu[...], preferred_element_type=jnp.float32) + bias[...]
        gated = (mixed[...].astype(jnp.float32) * jax.nn.sigmoid(pre)).astype(jnp.bfloat16)
        for copy in copies[1:]:
            copy.wait()
        stream = own[...].astype(jnp.float32) + jnp.dot(
            gated, branch[...], preferred_element_type=jnp.float32
        )
        out_stream[...] = stream
        out_normed[...] = row_norm(stream, gain[...])

    vmem = pl.BlockSpec(memory_space=pltpu.VMEM)
    return pl.pallas_call(
        kernel,
        in_specs=[vmem] * 3 + [pl.BlockSpec(memory_space=pl.ANY)] * 3,
        out_specs=[vmem, vmem],
        out_shape=[
            jax.ShapeDtypeStruct((rows, features), jnp.float32),
            jax.ShapeDtypeStruct((rows, features), jnp.bfloat16),
        ],
        scratch_shapes=[
            pltpu.VMEM((rows, width), jnp.bfloat16),
            pltpu.VMEM((rows, features), jnp.bfloat16),
            pltpu.VMEM(w_glu.shape, jnp.bfloat16),
            pltpu.VMEM(w_branch.shape, jnp.bfloat16),
            pltpu.SemaphoreType.DMA((3,)),
        ],
        compiler_params=pltpu.CompilerParams(vmem_limit_bytes=60 * 1024 * 1024),
        name="glu",
    )(blocks, b_glu.reshape(1, -1), norm_gain.reshape(1, -1), w_glu, w_branch, residual_in)


def place_sums(stream, chunks):
    planes = lax.axis_size("sp")
    rows, features = stream.shape
    size = features // planes
    half = size // 2
    flat = [value for unused, values in chunks for value in values]

    def kernel(stream_ref, *refs):
        at = (lax.axis_index("sp"), lax.axis_index("grp"))
        values, out, total = (list(refs[:-2]), refs[-2], refs[-1])
        total[...] = stream_ref[...]

        def add(value, source, target, length):
            spot = pl.ds(pl.multiple_of(target, LANES), length)
            total[:, spot] += value[:, pl.ds(source, length)].astype(jnp.float32)

        for distances, sums in chunks:
            for ahead in range(len(sums)):
                value, source = (values.pop(0), 0)
                for d in distances:
                    block = (at[0] + (ahead - d + planes)) % planes * size
                    if d == 0:
                        add(value, source, block, size)
                    else:
                        add(value, source, block + at[1] * half, half)
                        add(value, source + half, block + (1 - at[1]) * half, half)
                    source += size
        out[...] = total[...].astype(jnp.bfloat16)

    vmem = pl.BlockSpec(memory_space=pltpu.VMEM)
    return pl.pallas_call(
        kernel,
        in_specs=[vmem] * (1 + len(flat)),
        out_specs=vmem,
        out_shape=jax.ShapeDtypeStruct((rows, features), jnp.bfloat16),
        scratch_shapes=[pltpu.VMEM((rows, features), jnp.float32)],
        compiler_params=pltpu.CompilerParams(vmem_limit_bytes=8 * 1024 * 1024),
        name="place_sums",
    )(stream, *flat)


def feed_forward(stream, normed, wides, talls, units):
    planes = lax.axis_size("sp")
    tokens = [normed]
    for d in range(1, planes):
        tokens.append(hop(normed, "sp", d))
    others = []
    for d in range(planes):
        others.append(swap(tokens[d], "tp", 2))
    own_hidden, tokens = gate_up(tokens + others, wides, 0, units)
    other_hidden = gate_up(tokens, wides, 1, units)[0]
    order = list(range(1, planes))
    chunks = []
    for distances in ([0, 1], order[1:]):
        kept, sent = down((own_hidden, other_hidden), talls, distances)
        sent = swap(sent, "tp", 2)
        values = list(add_sums(kept, sent, planes))
        for d in range(1, planes):
            values[d] = hop(values[d], "sp", -d)
        chunks.append((distances, values))
    return place_sums(stream, chunks)


def per_device(
    ssm_input,
    residual_in,
    log_step,
    decay_real,
    freq,
    in_real,
    in_imag,
    out_real,
    out_imag,
    skip,
    w_glu,
    b_glu,
    w_branch,
    norm_gain,
    w_gate,
    w_up,
    w_down,
):
    tok_rows, width_local = ssm_input.shape
    group_count = log_step.shape[0]
    group_size = in_real.shape[2]
    tp_count = lax.axis_size("tp")
    tp_index = lax.axis_index("tp")
    own_rows = tok_rows // tp_count
    if can_reshard(tok_rows, group_count, in_real.shape, w_gate, w_down):
        wides, talls = reshard(w_gate, w_up, w_down)
        mixer_out = mixer(
            ssm_input, log_step, decay_real, freq, in_real, in_imag, out_real, out_imag, skip
        )
        blocks = lax.all_to_all(
            mixer_out.reshape(tp_count, own_rows, width_local), "tp", split_axis=0, concat_axis=0, tiled=True
        )
        stream, normed = gated_branch(blocks, w_glu, b_glu, w_branch, residual_in, norm_gain)
        return feed_forward(stream, normed, wides, talls, w_gate.shape[1])
    step_size, abar_re, _, bbar_re, bbar_im = discretize(
        log_step, decay_real, freq, in_real, in_imag
    )
    pow_re, pow_im = powers(decay_real, freq, step_size, tok_rows)
    inputs = ssm_input.astype(jnp.float32).reshape(tok_rows, group_count, group_size)
    local_re, local_im = local_states(inputs, decay_real, freq, step_size, bbar_re, bbar_im)
    identity = (
        jnp.ones_like(abar_re),
        jnp.zeros_like(abar_re),
        jnp.zeros_like(abar_re),
        jnp.zeros_like(abar_re),
    )
    carried = prefix((pow_re[-1], pow_im[-1], local_re[-1], local_im[-1]), "sp", compose, identity)
    state_re = local_re + pow_re * carried[2][None] - pow_im * carried[3][None]
    state_im = local_im + pow_re * carried[3][None] + pow_im * carried[2][None]
    mixer_out = readout(
        state_re, state_im, out_real, out_imag, skip.reshape(group_count, group_size), inputs
    )
    mixer_rows = lax.all_to_all(mixer_out, "tp", split_axis=0, concat_axis=1, tiled=True)
    glu_pre = jnp.dot(mixer_rows, w_glu, preferred_element_type=jnp.float32) + b_glu
    gated = (mixer_rows.astype(jnp.float32) * jax.nn.sigmoid(glu_pre)).astype(jnp.bfloat16)
    residual_own = lax.dynamic_slice_in_dim(residual_in, tp_index * own_rows, own_rows, 0)
    stream = residual_own.astype(jnp.float32) + jnp.dot(
        gated, w_branch, preferred_element_type=jnp.float32
    )
    normed = row_norm(stream, norm_gain)
    normed_all = lax.all_gather(normed, "tp", axis=0, tiled=True)
    gate_sum = jnp.dot(
        normed_all,
        lax.all_gather(w_gate, "sp", axis=0, tiled=True),
        preferred_element_type=jnp.float32,
    )
    up_sum = jnp.dot(
        normed_all,
        lax.all_gather(w_up, "sp", axis=0, tiled=True),
        preferred_element_type=jnp.float32,
    )
    hidden = (jax.nn.silu(gate_sum) * up_sum).astype(jnp.bfloat16)
    down_whole = lax.all_gather(w_down, "sp", axis=1, tiled=True)
    summed = lax.psum_scatter(
        jnp.dot(hidden, down_whole, preferred_element_type=jnp.float32).astype(jnp.bfloat16),
        "tp",
        scatter_dimension=0,
        tiled=True,
    ).astype(jnp.float32)
    return (stream + summed).astype(jnp.bfloat16)


def solution(mesh):
    placed = (
        P(("grp", "sp"), "tp"),
        P(("grp", "sp"), None),
        P("tp"),
        P("tp", None),
        P("tp", None),
        P("tp", None, None),
        P("tp", None, None),
        P("tp", None, None),
        P("tp", None, None),
        P("tp"),
        P(),
        P(),
        P(),
        P(),
        P("sp", "tp"),
        P("sp", "tp"),
        P("tp", "sp"),
    )

    return jax.shard_map(
        per_device,
        mesh=mesh,
        in_specs=placed,
        out_specs=P(("grp", "sp", "tp"), None),
        check_vma=False,
    )
```

```python
import math

import jax
import jax.numpy as jnp
from jax import lax
from jax.experimental import pallas as pl
from jax.experimental.pallas import tpu as pltpu
from jax.sharding import PartitionSpec as P

EPS = 1e-06


def prefix(shard, axis, combine, identity):
    count, place = (lax.axis_size(axis), lax.axis_index(axis))
    everything = tuple(jnp.moveaxis(lax.all_gather(jnp.stack(shard), axis), 1, 0))
    start = jax.tree.map(
        lambda part, zero: jnp.broadcast_to(jnp.asarray(zero, part.dtype), part.shape),
        shard,
        identity,
    )

    def lap(k, before):
        reached = k < place
        new = combine(before, tuple(part[k] for part in everything))
        return jax.tree.map(lambda a, b: jnp.where(reached, a, b), new, before)

    return lax.fori_loop(0, count, lap, start)


def discretize(log_step, decay_real, freq, in_real, in_imag):
    step_size = jnp.exp(log_step)[:, None]
    magnitude = jnp.exp(decay_real * step_size)
    abar_re = magnitude * jnp.cos(freq * step_size)
    abar_im = magnitude * jnp.sin(freq * step_size)
    denominator = decay_real * decay_real + freq * freq
    less_re = abar_re - 1.0
    hold_re = ((less_re * decay_real + abar_im * freq) / denominator)[..., None]
    hold_im = ((abar_im * decay_real - less_re * freq) / denominator)[..., None]
    bbar_re = hold_re * in_real - hold_im * in_imag
    bbar_im = hold_re * in_imag + hold_im * in_real
    return (step_size, abar_re, abar_im, bbar_re, bbar_im)


def powers(decay_real, freq, step_size, length):
    steps_up = (jnp.arange(length, dtype=jnp.int32) + 1).astype(jnp.float32)[:, None, None]
    magnitude = jnp.exp((decay_real * step_size)[None] * steps_up)
    phase = (freq * step_size)[None] * steps_up
    return (magnitude * jnp.cos(phase), magnitude * jnp.sin(phase))


def compose(earlier, later):
    a1r, a1i, b1r, b1i = earlier
    a2r, a2i, b2r, b2i = later
    return (
        a2r * a1r - a2i * a1i,
        a2r * a1i + a2i * a1r,
        a2r * b1r - a2i * b1i + b2r,
        a2r * b1i + a2i * b1r + b2i,
    )


def local_states(inputs, decay_real, freq, step_size, bbar_re, bbar_im):
    highest = lax.Precision.HIGHEST
    tok_rows, group_count, _ = inputs.shape
    lanes = group_count * decay_real.shape[1]
    drive_re = jnp.einsum("lgm,gpm->lgp", inputs, bbar_re, precision=highest).reshape(
        tok_rows, lanes
    )
    drive_im = jnp.einsum("lgm,gpm->lgp", inputs, bbar_im, precision=highest).reshape(
        tok_rows, lanes
    )
    span = math.gcd(tok_rows, 16)
    spans = tok_rows // span
    rate = (decay_real * step_size).reshape(lanes)
    turn = (freq * step_size).reshape(lanes)
    later = jnp.arange(span, dtype=jnp.int32)[:, None]
    earlier = jnp.arange(span, dtype=jnp.int32)[None, :]
    lag = (later - earlier).astype(jnp.float32)
    causal = (later >= earlier)[..., None]
    lag_pos = jnp.maximum(lag, 0.0)[..., None]
    table_mag = jnp.exp(rate[None, None] * lag_pos)
    table_re = jnp.where(causal, table_mag * jnp.cos(turn[None, None] * lag_pos), 0.0)
    table_im = jnp.where(causal, table_mag * jnp.sin(turn[None, None] * lag_pos), 0.0)
    block_re = drive_re.reshape(spans, 1, span, lanes)
    block_im = drive_im.reshape(spans, 1, span, lanes)
    inner_re = jnp.sum(table_re[None] * block_re - table_im[None] * block_im, axis=2)
    inner_im = jnp.sum(table_re[None] * block_im + table_im[None] * block_re, axis=2)
    steps_up = (jnp.arange(span, dtype=jnp.int32) + 1).astype(jnp.float32)[:, None]
    pow_mag = jnp.exp(rate[None] * steps_up)
    pow_re = pow_mag * jnp.cos(turn[None] * steps_up)
    pow_im = pow_mag * jnp.sin(turn[None] * steps_up)
    span_re = pow_re[-1]
    span_im = pow_im[-1]

    def carry_step(entering, ends):
        next_re = span_re * entering[0] - span_im * entering[1] + ends[0]
        next_im = span_re * entering[1] + span_im * entering[0] + ends[1]
        return ((next_re, next_im), entering)

    zeros = jnp.zeros((lanes,), jnp.float32)
    _, entering = lax.scan(
        carry_step, (zeros, zeros), (inner_re[:, -1], inner_im[:, -1])
    )
    state_re = inner_re + pow_re[None] * entering[0][:, None] - pow_im[None] * entering[1][:, None]
    state_im = inner_im + pow_re[None] * entering[1][:, None] + pow_im[None] * entering[0][:, None]
    shape = (tok_rows, group_count, decay_real.shape[1])
    return (state_re.reshape(shape), state_im.reshape(shape))


def readout(state_re, state_im, out_real, out_imag, skip_mat, inputs):
    highest = lax.Precision.HIGHEST
    values = (
        jnp.einsum("lgp,gmp->lgm", state_re, out_real, precision=highest)
        - jnp.einsum("lgp,gmp->lgm", state_im, out_imag, precision=highest)
        + skip_mat[None] * inputs
    )
    values = jax.nn.gelu(values)
    return values.reshape(values.shape[0], -1).astype(jnp.bfloat16)


def row_norm(stream, norm_gain):
    scale_rows = lax.rsqrt(jnp.mean(stream * stream, axis=-1, keepdims=True) + EPS)
    return (stream * scale_rows * norm_gain).astype(jnp.bfloat16)


LANES = 128


def can_reshard(tok_rows, group_count, in_shape, w_gate, w_down):
    planes, parts, cores = (lax.axis_size("sp"), lax.axis_size("grp"), lax.axis_size("tp"))
    rows, units = w_gate.shape
    width = tile_width(units, planes)
    return (
        2 < planes <= 8
        and parts == 2
        and cores == 4
        and units >= width
        and rows % (2 * LANES) == 0
        and w_down.shape[1] % (2 * LANES) == 0
        and tok_rows % (cores * 16) == 0
        and tok_rows & (tok_rows - 1) == 0
        and group_count * in_shape[1] % LANES == 0
        and group_count * in_shape[2] % LANES == 0
    )


def tile_width(units, planes):
    return -(-(-(-units // planes)) // LANES) * LANES


def hop(value, axis, distance):
    count = lax.axis_size(axis)
    return lax.ppermute(value, axis, [(i, (i + distance) % count) for i in range(count)])


def swap(value, axis, bit):
    return lax.ppermute(value, axis, [(i, i ^ bit) for i in range(lax.axis_size(axis))])


def halves(value):
    high = value.astype(jnp.bfloat16)
    return (high, (value - high.astype(jnp.float32)).astype(jnp.bfloat16))


def across(a, b):
    return lax.dot_general(a, b, (((1,), (1,)), ((), ())), preferred_element_type=jnp.float32)


def times(a, b):
    return (a[0] * b[0] - a[1] * b[1], a[0] * b[1] + a[1] * b[0])


def repeated(value, copies):
    size = value.shape[1]
    shape = (size, copies * size)
    pick = lax.broadcasted_iota(jnp.int32, shape, 0) == lax.broadcasted_iota(jnp.int32, shape, 1) % size
    return jnp.dot(value, pick.astype(jnp.bfloat16), preferred_element_type=jnp.float32)


def block_diagonal(value, groups):
    rows, size = (value.shape[0] // groups, value.shape[1])
    shape = (value.shape[0], groups * size)
    own = lax.broadcasted_iota(jnp.int32, shape, 0) // rows == lax.broadcasted_iota(jnp.int32, shape, 1) // size
    return [jnp.where(own, repeated(part, groups), 0.0).astype(jnp.bfloat16) for part in halves(value)]


def local_scan(ssm_input, log_step, decay_real, freq, in_real, in_imag):
    length = ssm_input.shape[0]
    groups, states, size = in_real.shape
    lanes = groups * states

    def kernel(log_ref, x, decay_ref, freq_ref, in_re, in_im, out_re, out_im, end, abar, hold):
        row = lax.broadcasted_iota(jnp.int32, (groups, states), 0)
        log = jnp.zeros((groups, states), jnp.float32)
        for g in range(groups):
            log = jnp.where(row == g, log_ref[g], log)
        step = jnp.exp(log)
        decay, turn = (decay_ref[...], freq_ref[...])
        magnitude = jnp.exp(decay * step)
        abar_re = magnitude * jnp.cos(turn * step)
        abar_im = magnitude * jnp.sin(turn * step)
        denominator = decay * decay + turn * turn
        less_re = abar_re - 1.0
        hold_re = (less_re * decay + abar_im * turn) / denominator
        hold_im = (abar_im * decay - less_re * turn) / denominator
        shape = (states, lanes)
        pick = lax.broadcasted_iota(jnp.int32, shape, 0) == lax.broadcasted_iota(jnp.int32, shape, 1) % states
        own = lax.broadcasted_iota(jnp.int32, (groups, lanes), 0) == (
            lax.broadcasted_iota(jnp.int32, (groups, lanes), 1) // states
        )
        for target, k, value in ((abar, 0, abar_re), (abar, 1, abar_im), (hold, 0, hold_re), (hold, 1, hold_im)):
            wide = jnp.dot(
                value, pick.astype(jnp.float32), preferred_element_type=jnp.float32, precision=lax.Precision.HIGHEST
            )
            target[k : k + 1, :] = jnp.sum(jnp.where(own, wide, 0.0), axis=0, keepdims=True)
        rows = x[...]
        for target, source in ((out_re, in_re), (out_im, in_im)):
            high, low = block_diagonal(source[...], groups)
            target[...] = jnp.dot(rows, high, preferred_element_type=jnp.float32) + jnp.dot(
                rows, low, preferred_element_type=jnp.float32
            )
        place = lax.broadcasted_iota(jnp.int32, (length, LANES), 0)
        for first in range(0, lanes, LANES):
            at = slice(first, first + LANES)
            power = (abar[0:1, at], abar[1:2, at])
            state = times((hold[0:1, at], hold[1:2, at]), (out_re[:, at], out_im[:, at]))
            gap = 1
            while gap < length:
                late = place >= gap
                before = tuple(jnp.where(late, pltpu.roll(part, gap, 0), 0.0) for part in state)
                moved = times(power, before)
                state = (state[0] + moved[0], state[1] + moved[1])
                power = times(power, power)
                gap *= 2
            out_re[:, at], out_im[:, at] = state
            end[0:1, at] = state[0][length - 1 :]
            end[1:2, at] = state[1][length - 1 :]

    pair = jax.ShapeDtypeStruct((2, lanes), jnp.float32)
    whole = jax.ShapeDtypeStruct((length, lanes), jnp.float32)
    vmem = pl.BlockSpec()
    return pl.pallas_call(
        kernel,
        grid=(1,),
        in_specs=[pl.BlockSpec(memory_space=pltpu.SMEM)] + [vmem] * 5,
        out_specs=[vmem] * 4,
        out_shape=[whole, whole, pair, pair],
        scratch_shapes=[pltpu.VMEM((2, lanes), jnp.float32)],
        compiler_params=pltpu.CompilerParams(vmem_limit_bytes=20 * 1024 * 1024),
        name="local_scan",
    )(
        log_step,
        ssm_input,
        decay_real,
        freq,
        jnp.swapaxes(in_real, 1, 2).reshape(groups * size, states),
        jnp.swapaxes(in_imag, 1, 2).reshape(groups * size, states),
    )


def mixed_out(state_re, state_im, abar, ends, out_real, out_imag, skip, ssm_input):
    length, lanes = state_re.shape
    groups, size, states = out_real.shape
    span = 8

    def kernel(*refs):
        s_re, s_im, abar_ref = refs[:3]
        end_refs = refs[3 : 3 + len(ends)]
        o_re, o_im, skip_ref, x, out = refs[3 + len(ends) : 8 + len(ends)]
        full_re, full_im = refs[8 + len(ends) :]
        for first in range(0, lanes, LANES):
            at = slice(first, first + LANES)
            one = (abar_ref[0:1, at], abar_ref[1:2, at])
            count = lax.broadcasted_iota(jnp.int32, (span, LANES), 0) + 1
            table = (jnp.ones((span, LANES), jnp.float32), jnp.zeros((span, LANES), jnp.float32))
            power, gap = (one, 1)
            while gap < length:
                if gap == span:
                    eight = power
                if gap <= span:
                    more = times(table, power)
                    odd = (count // gap) % 2 == 1
                    table = tuple(jnp.where(odd, a, b) for a, b in zip(more, table))
                power = times(power, power)
                gap *= 2
            carry = None
            for end in reversed(end_refs):
                here = (end[0:1, at], end[1:2, at])
                if carry is None:
                    carry = here
                else:
                    moved = times(power, carry)
                    carry = (here[0] + moved[0], here[1] + moved[1])
            table = times(table, carry)
            for start in range(0, length, span):
                rows = slice(start, start + span)
                full_re[rows, at] = s_re[rows, at] + table[0]
                full_im[rows, at] = s_im[rows, at] + table[1]
                table = times(table, eight)
        re_high, re_low = halves(full_re[...])
        im_high, im_low = halves(full_im[...])
        cre_high, cre_low = block_diagonal(o_re[...], groups)
        cim_high, cim_low = block_diagonal(o_im[...], groups)
        value = across(re_high, cre_high) + across(re_low, cre_high) + across(re_high, cre_low)
        value -= across(im_high, cim_high) + across(im_low, cim_high) + across(im_high, cim_low)
        value += skip_ref[...] * x[...].astype(jnp.float32)
        out[...] = jax.nn.gelu(value).astype(jnp.bfloat16)

    vmem = pl.BlockSpec()
    return pl.pallas_call(
        kernel,
        grid=(1,),
        in_specs=[vmem] * (7 + len(ends)),
        out_specs=vmem,
        out_shape=jax.ShapeDtypeStruct((length, groups * size), jnp.bfloat16),
        scratch_shapes=[pltpu.VMEM((length, lanes), jnp.float32)] * 2,
        compiler_params=pltpu.CompilerParams(vmem_limit_bytes=20 * 1024 * 1024),
        name="mixed_out",
    )(
        state_re,
        state_im,
        abar,
        *ends,
        out_real.reshape(groups * size, states),
        out_imag.reshape(groups * size, states),
        skip.reshape(1, -1),
        ssm_input,
    )


def mixer(ssm_input, log_step, decay_real, freq, in_real, in_imag, out_real, out_imag, skip):
    planes = lax.axis_size("sp")
    state_re, state_im, end, abar = local_scan(ssm_input, log_step, decay_real, freq, in_real, in_imag)
    ends = []
    for d in range(1, planes):
        ends.append(lax.ppermute(end, "sp", [(i, i + d) for i in range(planes - d)]))
    return mixed_out(state_re, state_im, abar, ends, out_real, out_imag, skip, ssm_input)


def first_unit(plane, planes, units):
    width = tile_width(units, planes)
    return jnp.minimum(plane * width, units - width)


def run_copies(copies, sems):
    copies = [pltpu.make_async_copy(a, b, sems.at[i]) for i, (a, b) in enumerate(copies)]
    for copy in copies:
        copy.start()
    for copy in copies:
        copy.wait()


def cut(w_gate, w_up, w_down, wide_at, tall_at, grant):
    planes = lax.axis_size("sp")
    rows, units = w_gate.shape
    cols = w_down.shape[1]
    width = tile_width(units, planes)
    count = len(wide_at)

    def kernel(gate, up, down, *refs):
        wides, talls = (refs[:count], refs[count:-1])
        place, part = (lax.axis_index("sp"), lax.axis_index("grp"))
        row = pl.ds(pl.multiple_of(part * (rows // 2), LANES), rows // 2)
        col = pl.ds(pl.multiple_of(part * (cols // 2), LANES), cols // 2)

        def units_of(d):
            first = first_unit((place + d) % planes, planes, units)
            return pl.ds(pl.multiple_of(first, LANES), width)

        copies = []
        for (d, what), wide in zip(wide_at, wides):
            r = row if d else slice(None)
            sources = [w for w, name in ((gate, "gate"), (up, "up")) if what in (name, "both")]
            for i, source in enumerate(sources):
                copies.append((source.at[r, units_of(d)], wide.at[:, pl.ds(i * width, width)]))
        for d, tall in zip(tall_at, talls):
            copies.append((down.at[units_of(d), col if d else slice(None)], tall))
        run_copies(copies, refs[-1])

    anywhere = pl.BlockSpec(memory_space=pltpu.HBM)
    shapes = [
        (rows // 2 if d else rows, 2 * width if what == "both" else width) for d, what in wide_at
    ]
    shapes += [(width, cols // 2 if d else cols) for d in tall_at]
    pieces = pl.pallas_call(
        kernel,
        in_specs=[anywhere] * 3,
        out_specs=[pl.BlockSpec(memory_space=pltpu.VMEM)] * len(shapes),
        out_shape=[jax.ShapeDtypeStruct(shape, w_gate.dtype) for shape in shapes],
        scratch_shapes=[pltpu.SemaphoreType.DMA((2 * count + len(tall_at),))],
        compiler_params=pltpu.CompilerParams(vmem_limit_bytes=grant * 1024 * 1024),
    )(w_gate, w_up, w_down)
    return (dict(zip(wide_at, pieces[:count])), dict(zip(tall_at, pieces[count:])))


def reshard(w_gate, w_up, w_down):
    planes = lax.axis_size("sp")
    order = list(range(1, planes))
    last = order[-1]
    first, unused = cut(w_gate, w_up, w_down, [(1, "both"), (last, "gate")], [], 60)
    middle = [(d, "both") for d in order[1:-1]] + [(last, "up")]
    second, unused = cut(w_gate, w_up, w_down, middle, [], 60)
    third, talls = cut(w_gate, w_up, w_down, [(0, "both")], order + [0], 60)

    def spread(piece, d):
        if d == 0:
            return [(piece, swap(piece, "tp", 1))]
        mine = hop(piece, "sp", d)
        other = swap(mine, "grp", 1)
        return [(half, swap(half, "tp", 1)) for half in (mine, other)]

    wides = []
    for (d, what), piece in {**first, **second, **third}.items():
        wides += [(d, what, half, pair) for half, pair in enumerate(spread(piece, d))]
    return (wides, {d: spread(piece, d) for d, piece in talls.items()})


def gate_up(tokens, wides, core, units):
    planes = lax.axis_size("sp")
    whole = not isinstance(tokens, list)
    toks = [tokens] if whole else tokens
    rows, features = toks[0].shape
    count = rows * len(toks)
    block = features // planes
    width = tile_width(units, planes)
    pieces = [pair[core] for unused_d, unused_what, unused_half, pair in wides]

    def kernel(*refs):
        place, part = (lax.axis_index("sp"), lax.axis_index("grp"))
        spots = []
        for d, what, half, unused in wides:
            start = (place - d + planes) % planes * block
            if d:
                start += (1 - part if half else part) * (block // 2)
            spots.append((start, width if what == "up" else 0))
        tok_refs, weights = (refs[: len(toks)], refs[len(toks) : len(toks) + len(pieces)])
        out, *outs, wide, sems = refs[len(toks) + len(pieces) :]
        tok = tok_refs[0] if whole else outs[0]
        moves = [] if whole else [(ref, tok.at[pl.ds(i * rows, rows), :]) for i, ref in enumerate(tok_refs)]
        later = []
        for (start, col), weight in zip(spots, weights):
            row = pl.ds(pl.multiple_of(start, 16), weight.shape[0])
            for first in range(0, weight.shape[1], width):
                part_of = weight.at[:, pl.ds(first, width)]
                target = wide.at[row, pl.ds(col + first, width)]
                (later if col + first else moves).append((part_of, target))
        count_first = len(moves)
        copies = [pltpu.make_async_copy(a, b, sems.at[i]) for i, (a, b) in enumerate(moves + later)]
        for copy in copies:
            copy.start()
        for copy in copies[:count_first]:
            copy.wait()
        gate = jnp.dot(tok[...], wide[:, :width], preferred_element_type=jnp.float32)
        for copy in copies[count_first:]:
            copy.wait()
        up = jnp.dot(tok[...], wide[:, width:], preferred_element_type=jnp.float32)
        hidden = gate / (1.0 + jnp.exp(-gate)) * up
        live = lax.broadcasted_iota(jnp.int32, hidden.shape, 1) >= place * width - first_unit(
            place, planes, units
        )
        out[...] = jnp.where(live, hidden, 0.0).astype(jnp.bfloat16)

    anywhere = pl.BlockSpec(memory_space=pl.ANY)
    vmem = pl.BlockSpec(memory_space=pltpu.VMEM)
    shapes = [jax.ShapeDtypeStruct((count, width), jnp.bfloat16)]
    if not whole:
        shapes.append(jax.ShapeDtypeStruct((count, features), jnp.bfloat16))
    return pl.pallas_call(
        kernel,
        in_specs=[vmem] * len(toks) + [anywhere] * len(pieces),
        out_specs=[vmem] * len(shapes),
        out_shape=shapes,
        scratch_shapes=[
            pltpu.VMEM((features, 2 * width), jnp.bfloat16),
            pltpu.SemaphoreType.DMA((len(toks) + 2 * len(pieces),)),
        ],
        compiler_params=pltpu.CompilerParams(vmem_limit_bytes=16 * 1024 * 1024),
    )(*toks, *pieces)


def down(hiddens, talls, distances):
    count, width = hiddens[0].shape
    pairs = [pair for d in distances for pair in talls[d]]
    flat = [piece for pair in pairs for piece in pair]
    cols = sum(own.shape[1] for own, unused in pairs)
    kept = count // 2

    def kernel(own_hidden, other_hidden, *refs):
        weights = refs[: len(flat)]
        out_kept, out_sent, tall, sems = refs[len(flat) :]
        copies, at = ([], 0)
        for i, (own, unused) in enumerate(pairs):
            col = pl.ds(at, own.shape[1])
            copies += [(weights[2 * i + core], tall.at[core, :, col]) for core in range(2)]
            at += own.shape[1]
        run_copies(copies, sems)

        def product(rows):
            return jnp.dot(
                own_hidden[rows, :], tall[0], preferred_element_type=jnp.float32
            ) + jnp.dot(other_hidden[rows, :], tall[1], preferred_element_type=jnp.float32)

        out_sent[...] = product(slice(kept, count)).astype(jnp.bfloat16)
        out_kept[...] = product(slice(0, kept))

    anywhere = pl.BlockSpec(memory_space=pl.ANY)
    vmem = pl.BlockSpec(memory_space=pltpu.VMEM)
    return pl.pallas_call(
        kernel,
        in_specs=[vmem] * 2 + [anywhere] * len(flat),
        out_specs=[vmem, vmem],
        out_shape=[
            jax.ShapeDtypeStruct((kept, cols), jnp.float32),
            jax.ShapeDtypeStruct((count - kept, cols), jnp.bfloat16),
        ],
        scratch_shapes=[
            pltpu.VMEM((2, width, cols), jnp.bfloat16),
            pltpu.SemaphoreType.DMA((len(flat),)),
        ],
        compiler_params=pltpu.CompilerParams(vmem_limit_bytes=16 * 1024 * 1024),
    )(*hiddens, *flat)


def add_sums(kept, sent, count):
    rows, cols = (kept.shape[0] // count, kept.shape[1])

    def kernel(a, b, *outs):
        for i, out in enumerate(outs):
            at = slice(i * rows, (i + 1) * rows)
            out[...] = (a[at, :] + b[at, :].astype(jnp.float32)).astype(out.dtype)

    vmem = pl.BlockSpec(memory_space=pltpu.VMEM)
    return pl.pallas_call(
        kernel,
        in_specs=[vmem, vmem],
        out_specs=[vmem] * count,
        out_shape=[jax.ShapeDtypeStruct((rows, cols), jnp.float32)]
        + [jax.ShapeDtypeStruct((rows, cols), jnp.bfloat16)] * (count - 1),
        compiler_params=pltpu.CompilerParams(vmem_limit_bytes=8 * 1024 * 1024),
    )(kept, sent)


def gated_branch(blocks, w_glu, b_glu, w_branch, residual_in, norm_gain):
    senders, rows, channels = blocks.shape
    width, features = w_branch.shape

    def kernel(block, bias, gain, glu_hbm, branch_hbm, residual, out_stream, out_normed, mixed, own, glu, branch, sems):
        at = pl.ds(pl.multiple_of(lax.axis_index("tp") * rows, 16), rows)
        copies = [(glu_hbm, glu), (branch_hbm, branch), (residual.at[at, :], own)]
        copies = [pltpu.make_async_copy(a, b, sems.at[i]) for i, (a, b) in enumerate(copies)]
        for copy in copies:
            copy.start()
        for i in range(senders):
            mixed[:, i * channels : (i + 1) * channels] = block[i]
        copies[0].wait()
        pre = jnp.dot(mixed[...], glu[...], preferred_element_type=jnp.float32) + bias[...]
        gated = (mixed[...].astype(jnp.float32) * jax.nn.sigmoid(pre)).astype(jnp.bfloat16)
        for copy in copies[1:]:
            copy.wait()
        stream = own[...].astype(jnp.float32) + jnp.dot(
            gated, branch[...], preferred_element_type=jnp.float32
        )
        out_stream[...] = stream
        out_normed[...] = row_norm(stream, gain[...])

    vmem = pl.BlockSpec(memory_space=pltpu.VMEM)
    return pl.pallas_call(
        kernel,
        in_specs=[vmem] * 3 + [pl.BlockSpec(memory_space=pl.ANY)] * 3,
        out_specs=[vmem, vmem],
        out_shape=[
            jax.ShapeDtypeStruct((rows, features), jnp.float32),
            jax.ShapeDtypeStruct((rows, features), jnp.bfloat16),
        ],
        scratch_shapes=[
            pltpu.VMEM((rows, width), jnp.bfloat16),
            pltpu.VMEM((rows, features), jnp.bfloat16),
            pltpu.VMEM(w_glu.shape, jnp.bfloat16),
            pltpu.VMEM(w_branch.shape, jnp.bfloat16),
            pltpu.SemaphoreType.DMA((3,)),
        ],
        compiler_params=pltpu.CompilerParams(vmem_limit_bytes=52 * 1024 * 1024),
        name="glu",
    )(blocks, b_glu.reshape(1, -1), norm_gain.reshape(1, -1), w_glu, w_branch, residual_in)


def place_sums(stream, chunks):
    planes = lax.axis_size("sp")
    rows, features = stream.shape
    size = features // planes
    half = size // 2
    flat = [value for unused, values in chunks for value in values]

    def kernel(stream_ref, *refs):
        at = (lax.axis_index("sp"), lax.axis_index("grp"))
        values, out, total = (list(refs[:-2]), refs[-2], refs[-1])
        total[...] = stream_ref[...]

        def add(value, source, target, length):
            spot = pl.ds(pl.multiple_of(target, LANES), length)
            total[:, spot] += value[:, pl.ds(source, length)].astype(jnp.float32)

        for distances, sums in chunks:
            for ahead in range(len(sums)):
                value, source = (values.pop(0), 0)
                for d in distances:
                    block = (at[0] + (ahead - d + planes)) % planes * size
                    if d == 0:
                        add(value, source, block, size)
                    else:
                        add(value, source, block + at[1] * half, half)
                        add(value, source + half, block + (1 - at[1]) * half, half)
                    source += size
        out[...] = total[...].astype(jnp.bfloat16)

    vmem = pl.BlockSpec(memory_space=pltpu.VMEM)
    return pl.pallas_call(
        kernel,
        in_specs=[vmem] * (1 + len(flat)),
        out_specs=vmem,
        out_shape=jax.ShapeDtypeStruct((rows, features), jnp.bfloat16),
        scratch_shapes=[pltpu.VMEM((rows, features), jnp.float32)],
        compiler_params=pltpu.CompilerParams(vmem_limit_bytes=8 * 1024 * 1024),
        name="place_sums",
    )(stream, *flat)


def feed_forward(stream, normed, wides, talls, units):
    planes = lax.axis_size("sp")
    tokens = [normed]
    for d in range(1, planes):
        tokens.append(hop(normed, "sp", d))
    others = []
    for d in range(planes):
        others.append(swap(tokens[d], "tp", 2))
    own_hidden, tokens = gate_up(tokens + others, wides, 0, units)
    other_hidden = gate_up(tokens, wides, 1, units)[0]
    order = list(range(1, planes))
    chunks = []
    for distances in ([0, 1], order[1:]):
        kept, sent = down((own_hidden, other_hidden), talls, distances)
        sent = swap(sent, "tp", 2)
        values = list(add_sums(kept, sent, planes))
        for d in range(1, planes):
            values[d] = hop(values[d], "sp", -d)
        chunks.append((distances, values))
    return place_sums(stream, chunks)


def per_device(
    ssm_input,
    residual_in,
    log_step,
    decay_real,
    freq,
    in_real,
    in_imag,
    out_real,
    out_imag,
    skip,
    w_glu,
    b_glu,
    w_branch,
    norm_gain,
    w_gate,
    w_up,
    w_down,
):
    tok_rows, width_local = ssm_input.shape
    group_count = log_step.shape[0]
    group_size = in_real.shape[2]
    tp_count = lax.axis_size("tp")
    tp_index = lax.axis_index("tp")
    own_rows = tok_rows // tp_count
    if can_reshard(tok_rows, group_count, in_real.shape, w_gate, w_down):
        wides, talls = reshard(w_gate, w_up, w_down)
        mixer_out = mixer(
            ssm_input, log_step, decay_real, freq, in_real, in_imag, out_real, out_imag, skip
        )
        blocks = lax.all_to_all(
            mixer_out.reshape(tp_count, own_rows, width_local), "tp", split_axis=0, concat_axis=0, tiled=True
        )
        stream, normed = gated_branch(blocks, w_glu, b_glu, w_branch, residual_in, norm_gain)
        return feed_forward(stream, normed, wides, talls, w_gate.shape[1])
    step_size, abar_re, _, bbar_re, bbar_im = discretize(
        log_step, decay_real, freq, in_real, in_imag
    )
    pow_re, pow_im = powers(decay_real, freq, step_size, tok_rows)
    inputs = ssm_input.astype(jnp.float32).reshape(tok_rows, group_count, group_size)
    local_re, local_im = local_states(inputs, decay_real, freq, step_size, bbar_re, bbar_im)
    identity = (
        jnp.ones_like(abar_re),
        jnp.zeros_like(abar_re),
        jnp.zeros_like(abar_re),
        jnp.zeros_like(abar_re),
    )
    carried = prefix((pow_re[-1], pow_im[-1], local_re[-1], local_im[-1]), "sp", compose, identity)
    state_re = local_re + pow_re * carried[2][None] - pow_im * carried[3][None]
    state_im = local_im + pow_re * carried[3][None] + pow_im * carried[2][None]
    mixer_out = readout(
        state_re, state_im, out_real, out_imag, skip.reshape(group_count, group_size), inputs
    )
    mixer_rows = lax.all_to_all(mixer_out, "tp", split_axis=0, concat_axis=1, tiled=True)
    glu_pre = jnp.dot(mixer_rows, w_glu, preferred_element_type=jnp.float32) + b_glu
    gated = (mixer_rows.astype(jnp.float32) * jax.nn.sigmoid(glu_pre)).astype(jnp.bfloat16)
    residual_own = lax.dynamic_slice_in_dim(residual_in, tp_index * own_rows, own_rows, 0)
    stream = residual_own.astype(jnp.float32) + jnp.dot(
        gated, w_branch, preferred_element_type=jnp.float32
    )
    normed = row_norm(stream, norm_gain)
    normed_all = lax.all_gather(normed, "tp", axis=0, tiled=True)
    gate_sum = jnp.dot(
        normed_all,
        lax.all_gather(w_gate, "sp", axis=0, tiled=True),
        preferred_element_type=jnp.float32,
    )
    up_sum = jnp.dot(
        normed_all,
        lax.all_gather(w_up, "sp", axis=0, tiled=True),
        preferred_element_type=jnp.float32,
    )
    hidden = (jax.nn.silu(gate_sum) * up_sum).astype(jnp.bfloat16)
    down_whole = lax.all_gather(w_down, "sp", axis=1, tiled=True)
    summed = lax.psum_scatter(
        jnp.dot(hidden, down_whole, preferred_element_type=jnp.float32).astype(jnp.bfloat16),
        "tp",
        scatter_dimension=0,
        tiled=True,
    ).astype(jnp.float32)
    return (stream + summed).astype(jnp.bfloat16)


def solution(mesh):
    placed = (
        P(("grp", "sp"), "tp"),
        P(("grp", "sp"), None),
        P("tp"),
        P("tp", None),
        P("tp", None),
        P("tp", None, None),
        P("tp", None, None),
        P("tp", None, None),
        P("tp", None, None),
        P("tp"),
        P(),
        P(),
        P(),
        P(),
        P("sp", "tp"),
        P("sp", "tp"),
        P("tp", "sp"),
    )

    return jax.shard_map(
        per_device,
        mesh=mesh,
        in_specs=placed,
        out_specs=P(("grp", "sp", "tp"), None),
        check_vma=False,
    )
```
